128 devices in a mesh: ep: 128 (over z, y, x, core).
Axes of the slice: x: 4, y: 4, z: 4, core: 2. Of those that a mesh axis runs over, the one named last changes fastest.
Arguments:
- hidden: bfloat16 [4096, 2048], P('ep'), may hold values from -6 to 6
- cache_keys: bfloat16 [4096, 1024, 128], P('ep'), may hold values from -512 to 512
- cache_values: bfloat16 [4096, 1024, 128], P('ep'), may hold values from -6 to 6
- lengths: int32 [4096], P('ep'), may hold values from 1 to 1024
- first_gain: float32 [2048], replicated, may hold values from 0.1 to 1.9
- query_weight: bfloat16 [2048, 1024], replicated, may hold values from -0.125 to 0.125
- key_weight: bfloat16 [2048, 128], replicated, may hold values from -0.125 to 0.125
- value_weight: bfloat16 [2048, 128], replicated, may hold values from -0.125 to 0.125
- mixing: float32 [8], replicated, may hold values from 0.3 to 0.8
- head_gain: float32 [128], replicated, may hold values from 0.1 to 1.9
- out_weight: bfloat16 [1024, 2048], replicated, may hold values from -0.1875 to 0.1875
- second_gain: float32 [2048], replicated, may hold values from 0.1 to 1.9
- routes: int32 [4096, 4], P('ep'), may hold values from 0 to 63, as said below
- route_weight: float32 [4096, 4], P('ep'), may hold values from 0.05 to 1
- expert_gate: bfloat16 [128, 2048, 256], P('ep'), may hold values from -0.125 to 0.125
- expert_up: bfloat16 [128, 2048, 256], P('ep'), may hold values from -0.125 to 0.125
- expert_down: bfloat16 [128, 256, 2048], P('ep'), may hold values from -0.25 to 0.25
Outputs:
- layer_out: bfloat16 [4096, 2048], P('ep')
- new_key: bfloat16 [4096, 128], P('ep')
- new_value: bfloat16 [4096, 128], P('ep')
The draws below stay inside these ranges and needn't reach their ends.
Inputs may be any that keep to these rules, and one draw needn't show every extreme that they name: `routes`: each row names 4 different experts of one group, that is of one block of 16 consecutive numbers. Among the rows of one device, two rows name the same set of experts or disjoint sets, and no expert is named by more than 4 rows; one and the same expert is named by exactly 4 rows on every device.
All inputs are finite; a program needn't handle non-finite values.
Results may differ from the reference program's by a relative error of at most 0.025.
Values may be sent and summed in bfloat16 or wider, within the bound.
A program may use at most 128 MiB of HBM per device.

```python
import math
import jax
import jax.numpy as jnp
from jax import lax

D = 2048
HEADS = 8
DK = 64
DV = 128
D_EXPERT = 512
GROUPS = 4
EXP_SPLIT = 2
TOP_K = 4
SEQ_DEV = 32
LEN = 1024
TOKENS = 4096
EXPERTS = 64
EXP_GROUP = 16
CAP = 4


def draw_cache_keys(key, part):
    first = jax.random.fold_in(jax.random.fold_in(key, 3), 0)
    base = 1.8 * jnp.clip(jax.random.normal(first, (TOKENS, LEN, 2 * DK), jnp.float32), -6.0, 6.0)
    return base.astype(jnp.bfloat16)


def draw_routes(key, part):
    blocks = TOKENS // SEQ_DEV
    sets_group = EXP_GROUP // TOP_K
    set_count = EXPERTS // TOP_K
    tickets = set_count * CAP
    base = jax.random.fold_in(key, 7)
    star = jax.random.randint(jax.random.fold_in(base, 1), (), 0, EXPERTS).astype(jnp.int32)
    star_group = star // EXP_GROUP
    star_inner = star % EXP_GROUP

    def one_block(block_key):
        key_perm, key_order, key_rows = jax.random.split(block_key, 3)
        inner = jax.vmap(lambda part_key: jax.random.permutation(part_key, EXP_GROUP))(jax.random.split(key_perm, GROUPS)).astype(jnp.int32)
        members = inner + (jnp.arange(GROUPS, dtype=jnp.int32) * EXP_GROUP)[:, None]
        members = members.reshape(set_count, TOP_K)
        star_slot = jnp.sum(jnp.where(inner[star_group] == star_inner, jnp.arange(EXP_GROUP, dtype=jnp.int32), 0))
        star_set = star_group * sets_group + star_slot // TOP_K
        ticket_set = jnp.arange(tickets, dtype=jnp.int32) // CAP
        ranks = jax.random.permutation(key_order, tickets).astype(jnp.int32)
        sort_key = jnp.where(ticket_set == star_set, ranks - tickets, ranks)
        chosen = ticket_set[jnp.argsort(sort_key)[:SEQ_DEV]]
        rows = members[chosen]
        shuffle = jax.vmap(lambda row_key: jax.random.permutation(row_key, TOP_K))(jax.random.split(key_rows, SEQ_DEV)).astype(jnp.int32)
        return jnp.take_along_axis(rows, shuffle, axis=1)
    block_keys = jax.random.split(jax.random.fold_in(base, 2), blocks)
    return jax.vmap(one_block)(block_keys).reshape(TOKENS, TOP_K).astype(jnp.int32)


def place_ends(array, key, low, largest):
    dims = array.shape
    index_at = [jax.random.randint(jax.random.fold_in(key, axis), (), 0, dims[axis]) for axis in range(len(dims))]
    array = array.at[tuple(index_at)].set(low)
    longest = dims.index(max(dims))
    index_at[longest] = (index_at[longest] + 1) % dims[longest]
    return array.at[tuple(index_at)].set(largest)


def block_levels(own_key, shape, cuts, low, largest):
    level, own = 1.0, jax.random.fold_in(own_key, 6)
    for axis_at, shards_of in cuts:
        heights = jnp.exp(jax.random.uniform(jax.random.fold_in(own, axis_at), (shards_of,), jnp.float32, low / len(cuts), largest / len(cuts)))
        level = level * jnp.repeat(heights, shape[axis_at] // shards_of).reshape([-1 if axis == axis_at else 1 for axis in range(len(shape))])
    return level


def normal_values(stream_key, dims, deviation, limit, cuts=(), kind=jnp.bfloat16):
    entries = deviation * jax.random.normal(stream_key, dims, jnp.float32)
    if cuts:
        entries = entries * block_levels(stream_key, dims, cuts, -0.22, 0.18)
    return jnp.clip(entries, -limit, limit).astype(kind)


def setup_inputs(seed: int = 0) -> dict:
    key_of = jax.random.split(jax.random.key(seed), 18)
    hidden = normal_values(key_of[0], (TOKENS, D), 1.0, 6.0, ((0, 128),))
    cache_keys = draw_cache_keys(jax.random.fold_in(key_of[17], 71), 0)
    cache_values = normal_values(key_of[2], (TOKENS, LEN, DV), 1.0, 6.0, ((0, 128),))
    lengths = place_ends(jax.random.randint(key_of[3], (TOKENS,), 1, LEN + 1), jax.random.fold_in(key_of[3], 1), 1, LEN).astype(jnp.int32)
    first_gain = jnp.clip(1.0 + 0.18 * jax.random.normal(key_of[4], (D,), jnp.float32), 0.1, 1.9)
    query_weight = normal_values(key_of[5], (D, HEADS * 2 * DK), D ** -0.5, 0.125)
    key_weight = normal_values(key_of[6], (D, 2 * DK), D ** -0.5, 0.125)
    value_weight = normal_values(key_of[7], (D, DV), D ** -0.5, 0.125)
    mixing = jnp.clip(jax.random.uniform(key_of[8], (HEADS,), jnp.float32, 0.3, 0.8), 0.3, 0.8)
    head_gain = jnp.clip(1.0 + 0.18 * jax.random.normal(key_of[9], (DV,), jnp.float32), 0.1, 1.9)
    out_weight = normal_values(key_of[10], (HEADS * DV, D), (HEADS * DV) ** -0.5, 0.1875)
    second_gain = jnp.clip(1.0 + 0.18 * jax.random.normal(key_of[11], (D,), jnp.float32), 0.1, 1.9)
    routes = draw_routes(jax.random.fold_in(key_of[17], 71), 0)
    route_weight = jnp.clip(jnp.exp(math.log(1.0) - 2.9957323 * jax.random.uniform(key_of[13], (TOKENS, TOP_K), jnp.float32) ** block_levels(key_of[13], (TOKENS, TOP_K), ((0, 128),), -0.2, 0.2)), 0.05, 1.0)
    expert_gate = normal_values(key_of[14], (EXPERTS * EXP_SPLIT, D, D_EXPERT // EXP_SPLIT), D ** -0.5, 0.125, ((0, 128),))
    expert_up = normal_values(key_of[15], (EXPERTS * EXP_SPLIT, D, D_EXPERT // EXP_SPLIT), D ** -0.5, 0.125, ((0, 128),))
    expert_down = normal_values(key_of[16], (EXPERTS * EXP_SPLIT, D_EXPERT // EXP_SPLIT, D), D_EXPERT ** -0.5, 0.25, ((0, 128),))
    return {"hidden": hidden, "cache_keys": cache_keys, "cache_values": cache_values, "lengths": lengths, "first_gain": first_gain, "query_weight": query_weight, "key_weight": key_weight, "value_weight": value_weight, "mixing": mixing, "head_gain": head_gain, "out_weight": out_weight, "second_gain": second_gain, "routes": routes, "route_weight": route_weight, "expert_gate": expert_gate, "expert_up": expert_up, "expert_down": expert_down}


epsilon = 1e-06

def root_scale(rows, gain):
    values = rows.astype(jnp.float32)
    factor = lax.rsqrt(lax.optimization_barrier(jnp.mean(values * values, axis=-1, keepdims=True)) + epsilon)
    return values * factor * gain

def slot_tables(routes, experts, capacity):
    count, picks = routes.shape
    flat = routes.reshape(count * picks)
    indicator = (flat[:, None] == jnp.arange(experts, dtype=jnp.int32)[None, :]).astype(jnp.int32)
    before = jnp.cumsum(indicator, axis=0) - indicator
    place = lax.optimization_barrier(jnp.sum(before * indicator, axis=1))
    target = flat * capacity + place
    slots = jnp.arange(experts * capacity, dtype=jnp.int32)
    match = target[None, :] == slots[:, None]
    return match.reshape(experts * capacity, count, picks)

def attend(query, new_key, new_value, cache_keys, cache_values, lengths, mixing):
    count = query.shape[0]
    span = cache_keys.shape[1]
    queries = query.reshape(count, HEADS, 2, DK)
    keys = cache_keys.reshape(count, span, 2, DK)
    scores = jnp.einsum('shmd,slmd->shml', queries.astype(jnp.float32), keys.astype(jnp.float32)) * DK ** (-0.5)
    own_scores = jnp.einsum('shmd,smd->shm', queries.astype(jnp.float32), new_key.reshape(count, 2, DK).astype(jnp.float32)) * DK ** (-0.5)
    valid = jnp.arange(span, dtype=jnp.int32)[None, :] < lengths[:, None]
    scores = jnp.where(valid[:, None, None, :], scores, -jnp.inf)
    highest = jnp.maximum(lax.optimization_barrier(jnp.max(scores, axis=-1)), own_scores)
    weights = jnp.exp(scores - highest[..., None])
    own_weights = jnp.exp(own_scores - highest)
    total = lax.optimization_barrier(jnp.sum(weights, axis=-1)) + own_weights
    weights = weights / total[..., None]
    own_weights = own_weights / total
    contrast = (weights[:, :, 0] - mixing[None, :, None] * weights[:, :, 1]).astype(jnp.bfloat16)
    own_contrast = (own_weights[:, :, 0] - mixing[None, :] * own_weights[:, :, 1]).astype(jnp.bfloat16)
    mixed = jnp.einsum('shl,sle->she', contrast.astype(jnp.float32), cache_values.astype(jnp.float32))
    return mixed + own_contrast.astype(jnp.float32)[..., None] * new_value.astype(jnp.float32)[:, None, :]

def head_norm(mixed, head_gain):
    factor = lax.rsqrt(lax.optimization_barrier(jnp.mean(mixed * mixed, axis=-1, keepdims=True)) + epsilon)
    scaled = mixed * factor * head_gain
    return scaled.reshape(mixed.shape[0], HEADS * DV).astype(jnp.bfloat16)

def reference(hidden, cache_keys, cache_values, lengths, first_gain, query_weight, key_weight, value_weight, mixing, head_gain, out_weight, second_gain, routes, route_weight, expert_gate, expert_up, expert_down):
    normed = root_scale(hidden, first_gain).astype(jnp.bfloat16)
    query = jnp.dot(normed, query_weight, preferred_element_type=jnp.float32).astype(jnp.bfloat16)
    new_key = jnp.dot(normed, key_weight, preferred_element_type=jnp.float32).astype(jnp.bfloat16)
    new_value = jnp.dot(normed, value_weight, preferred_element_type=jnp.float32).astype(jnp.bfloat16)
    mixed = attend(query, new_key, new_value, cache_keys, cache_values, lengths, mixing)
    head_rows = head_norm(mixed, head_gain)
    update = jnp.dot(head_rows, out_weight, preferred_element_type=jnp.float32)
    residual = (hidden.astype(jnp.float32) + update).astype(jnp.bfloat16)
    expert_input = root_scale(residual, second_gain).astype(jnp.bfloat16)
    blocks = TOKENS // SEQ_DEV
    match = jax.vmap(lambda block: slot_tables(block, EXPERTS, CAP))(routes.reshape(blocks, SEQ_DEV, TOP_K))
    pick = lax.optimization_barrier(jnp.sum(match.astype(jnp.float32), axis=3))
    packed = jnp.einsum('bjs,bsd->bjd', pick, expert_input.reshape(blocks, SEQ_DEV, D).astype(jnp.float32))
    packed = packed.astype(jnp.bfloat16).reshape(blocks, EXPERTS, CAP, D)

    def one_expert(index):
        rows = lax.dynamic_index_in_dim(packed, index, 1, keepdims=False).reshape(blocks * CAP, D)
        summed = jnp.zeros((blocks * CAP, D), jnp.float32)
        for share in range(EXP_SPLIT):
            part = index * EXP_SPLIT + share
            gate = jnp.dot(rows, expert_gate[part], preferred_element_type=jnp.float32)
            upper = jnp.dot(rows, expert_up[part], preferred_element_type=jnp.float32)
            inner = (jax.nn.silu(gate) * upper).astype(jnp.bfloat16)
            result = jnp.dot(inner, expert_down[part], preferred_element_type=jnp.float32).astype(jnp.bfloat16)
            summed = summed + result.astype(jnp.float32)
        return summed.reshape(blocks, CAP, D)
    outputs = lax.map(one_expert, jnp.arange(EXPERTS, dtype=jnp.int32))
    outputs = jnp.moveaxis(outputs, 0, 1).reshape(blocks, EXPERTS * CAP, D)
    weighting = lax.optimization_barrier(jnp.sum(jnp.where(match, route_weight.reshape(blocks, 1, SEQ_DEV, TOP_K), 0.0), axis=3))
    routed = jnp.einsum('bjs,bjd->bsd', weighting, outputs, precision=lax.Precision.HIGHEST)
    layer_out = (residual.astype(jnp.float32) + routed.reshape(TOKENS, D)).astype(jnp.bfloat16)
    return (layer_out, new_key, new_value)
```

```python
import functools

import jax
import jax.numpy as jnp
from jax import lax
from jax.experimental import pallas as pl
from jax.experimental.pallas import tpu as pltpu
from jax.sharding import PartitionSpec as P

MESH = pl.DeviceIdType.MESH
BF16 = jnp.bfloat16
F32 = jnp.float32

D = 2048
HEADS = 8
DK = 64
DV = 128
PART = 256
TOP_K = 4
SEQS = 32
SPAN = 1024
CAP = 4
CHIPS = 64
SIDE = 4
GROUP = 8
GROUPS = SEQS // GROUP
WCHUNKS = 4
PIECES = 2
WIDTH = D // PIECES
ROWS = CAP * PIECES
BLOCKS = 4
PER = CHIPS // BLOCKS
MUL = 37
INV = pow(MUL, -1, CHIPS)
LANES = GROUP * HEADS * 2
EPS = 1e-06


def dot(a, b, dims=((1,), (0,))):
    return lax.dot_general(a, b, (dims, ((), ())), preferred_element_type=F32)


def iota(shape, axis):
    return lax.broadcasted_iota(jnp.int32, shape, axis)


def row_scale(values):
    return lax.rsqrt(jnp.mean(values * values, axis=-1, keepdims=True) + EPS)


def kernel(
    hidden_h, keys_h, values_h, lengths_h, gain1_h, wq_h, wk_h, wv_h, mixing_h, hgain_h, wo_h, gain2_h,
    routes_h, rweight_h, gate_h, up_h, down_h,
    out_h, nkey_h, nvalue_h,
    hidden, kbuf, vbuf, lens, gain1, wq, wk, wv, mixing, hgain, wo, gain2, routes, rweight, wg, wu, wd,
    qbuf, nkbuf, nvbuf, scores, contrast, heads, resid, outbuf, nkout, nvout,
    wcomb, sendbuf, recvbuf, ybuf, retbuf,
    small_sem, wq_sem, k_sem, v_sem, wo_sem, exp_sem, out_sem,
    wsend_sem, wrecv_sem, dsend_sem, drecv_sem, rsend_sem, rrecv_sem,
):
    me = lax.axis_index("ep")
    core = lax.rem(me, 2)
    chip = lax.div(me, 2)
    cx = lax.rem(chip, SIDE)
    cy = lax.rem(lax.div(chip, SIDE), SIDE)
    cz = lax.div(chip, SIDE * SIDE)
    sibling = chip * 2 + (1 - core)

    def partner(k, sign):
        rel = lax.rem(k * INV, CHIPS)
        dx = lax.rem(rel, SIDE)
        dy = lax.rem(lax.div(rel, SIDE), SIDE)
        dz = lax.div(rel, SIDE * SIDE)
        x = lax.rem(cx + sign * dx + SIDE, SIDE)
        y = lax.rem(cy + sign * dy + SIDE, SIDE)
        z = lax.rem(cz + sign * dz + SIDE, SIDE)
        return ((z * SIDE + y) * SIDE + x) * 2 + core

    barrier = pltpu.get_barrier_semaphore()

    def greet(k, carry):
        pl.semaphore_signal(barrier, inc=1, device_id=(partner(k, 1),), device_id_type=MESH)
        return carry

    lax.fori_loop(1, CHIPS, greet, 0)
    pl.semaphore_signal(barrier, inc=1, device_id=(sibling,), device_id_type=MESH)

    smalls = [
        (hidden_h, hidden), (gain1_h, gain1), (wk_h, wk), (wv_h, wv), (lengths_h, lens), (mixing_h, mixing),
        (hgain_h, hgain), (gain2_h, gain2), (routes_h, routes), (rweight_h, rweight),
    ]
    small = [pltpu.make_async_copy(a, b, small_sem.at[i]) for i, (a, b) in enumerate(smalls)]
    small[0].start()
    small[1].start()
    step = D // WCHUNKS
    wq_copies = [
        pltpu.make_async_copy(wq_h.at[pl.ds(i * step, step)], wq.at[pl.ds(i * step, step)], wq_sem.at[i])
        for i in range(WCHUNKS)
    ]
    for copy in wq_copies:
        copy.start()
    for copy in small[2:]:
        copy.start()

    def fetch(g, carry):
        for s in range(GROUP):
            pltpu.make_async_copy(keys_h.at[g * GROUP + s], kbuf.at[g, :, pl.ds(s * 2 * DK, 2 * DK)], k_sem.at[g]).start()
        for s in range(GROUP):
            pltpu.make_async_copy(values_h.at[g * GROUP + s], vbuf.at[g, :, pl.ds(s * DV, DV)], v_sem.at[g]).start()
        return carry

    own = [
        pltpu.make_async_copy(gate_h.at[0], wg.at[core], exp_sem.at[0]),
        pltpu.make_async_copy(up_h.at[0], wu.at[core], exp_sem.at[1]),
        pltpu.make_async_copy(down_h.at[0], wd.at[core], exp_sem.at[2]),
    ]
    wo_copy = pltpu.make_async_copy(wo_h, wo, wo_sem)
    fetch(0, 0)
    for copy in own:
        copy.start()
    lax.fori_loop(1, GROUPS, fetch, 0)
    wo_copy.start()

    small[0].wait()
    small[1].wait()
    values = hidden[...].astype(F32)
    normed = (values * row_scale(values) * gain1[...]).astype(BF16)
    query = jnp.zeros((SEQS, HEADS * 2 * DK), F32)
    for i in range(WCHUNKS):
        wq_copies[i].wait()
        query += dot(normed[:, i * step : (i + 1) * step], wq[i * step : (i + 1) * step, :])
    qbuf[...] = query.astype(BF16).astype(F32) * DK ** (-0.5)
    for copy in small[2:]:
        copy.wait()
    new_key = dot(normed, wk[...]).astype(BF16)
    new_value = dot(normed, wv[...]).astype(BF16)
    nkout[...] = new_key
    nvout[...] = new_value
    nkbuf[...] = new_key.astype(F32)
    nvbuf[...] = new_value.astype(F32)
    key_copy = pltpu.make_async_copy(nkout, nkey_h, out_sem.at[0])
    value_copy = pltpu.make_async_copy(nvout, nvalue_h, out_sem.at[1])
    key_copy.start()
    value_copy.start()

    lanes = PIECES * SEQS
    spread = (iota((SEQS, lanes), 0) == lax.rem(iota((SEQS, lanes), 1), SEQS)).astype(BF16)
    picks = dot(routes[...].astype(F32).astype(BF16), spread).astype(jnp.int32)
    lowest = jnp.min(picks, axis=0, keepdims=True)
    named = (iota((CHIPS, lanes), 0) == lowest).astype(F32)
    earlier = (iota((lanes, lanes), 0) < lax.rem(iota((lanes, lanes), 1), SEQS)).astype(F32)
    before = dot(named.astype(BF16), earlier.astype(BF16))
    place = jnp.sum(before * named, axis=0, keepdims=True).astype(jnp.int32)
    ex = lax.rem(picks, SIDE)
    ey = lax.rem(lax.div(picks, SIDE), SIDE)
    ez = lax.div(picks, SIDE * SIDE)
    offset = (
        lax.rem(ez - cz + SIDE, SIDE) * (SIDE * SIDE) + lax.rem(ey - cy + SIDE, SIDE) * SIDE + lax.rem(ex - cx + SIDE, SIDE)
    )
    piece = lax.div(iota((1, lanes), 1), SEQS)
    target = lax.rem(offset * MUL, CHIPS) * ROWS + piece * CAP + place
    high = rweight[...].astype(BF16)
    low = (rweight[...] - high.astype(F32)).astype(BF16)
    high = dot(high, spread)
    low = dot(low, spread)
    slot = iota((CHIPS * ROWS, lanes), 0)
    pick = jnp.zeros((CHIPS * ROWS, lanes), F32)
    comb_high = jnp.zeros((CHIPS * ROWS, lanes), F32)
    comb_low = jnp.zeros((CHIPS * ROWS, lanes), F32)
    for k in range(TOP_K):
        hit = slot == target[k : k + 1, :]
        pick = jnp.where(hit, 1.0, pick)
        comb_high = jnp.where(hit, high[k : k + 1, :], comb_high)
        comb_low = jnp.where(hit, low[k : k + 1, :], comb_low)
    pick = pick.astype(BF16)
    wcomb[...] = jnp.transpose(jnp.concatenate([comb_high, comb_low], axis=1)).astype(BF16)

    pl.semaphore_wait(barrier, CHIPS)

    def share(source, index):
        return pltpu.make_async_remote_copy(
            src_ref=source.at[core], dst_ref=source.at[core], send_sem=wsend_sem.at[index],
            recv_sem=wrecv_sem.at[index], device_id=(sibling,), device_id_type=MESH,
        )

    lane = iota((1, LANES), 1)
    lane_seq = lax.rem(lane, GROUP)
    lane_head = lax.rem(lax.div(lane, GROUP), HEADS)
    mix = jnp.zeros((1, LANES), F32)
    for h in range(HEADS):
        mix = jnp.where(lane_head == h, mixing[h], mix)
    mix = jnp.where(lane < LANES // 2, 1.0, mix)
    row = iota((LANES, 2 * DK), 0)
    col = iota((LANES, 2 * DK), 1)
    same_map = lax.div(row, LANES // 2) == lax.div(col, DK)
    row_seq = lax.rem(row, GROUP)

    def attend(g, carry):
        first = pl.multiple_of(g * GROUP, GROUP)
        rows = [qbuf[pl.ds(first, GROUP), h * 2 * DK : (h + 1) * 2 * DK] for h in range(HEADS)]
        block = jnp.concatenate(rows + rows, axis=0)
        block = jnp.where(same_map, block, 0.0)
        diag = jnp.concatenate(
            [jnp.where(row_seq == s, block, 0.0).astype(BF16) for s in range(GROUP)], axis=1
        )
        limit = jnp.zeros((1, LANES), jnp.int32)
        for s in range(GROUP):
            limit = jnp.where(lane_seq == s, lens[g * GROUP + s], limit)
        fresh = nkbuf[pl.ds(first, GROUP), :]
        fresh_rows = jnp.concatenate(
            [jnp.where(iota((GROUP, 2 * DK), 0) == s, fresh, 0.0).astype(BF16) for s in range(GROUP)], axis=1
        )
        own_score = jnp.sum(dot(fresh_rows, diag, ((1,), (1,))), axis=0, keepdims=True)
        pltpu.make_async_copy(kbuf.at[g], kbuf.at[g], k_sem.at[g]).wait()
        score = dot(kbuf[g], diag, ((1,), (1,)))
        score = jnp.where(iota((SPAN, LANES), 0) < limit, score, -jnp.inf)
        scores[...] = score
        highest = jnp.maximum(jnp.max(score, axis=0, keepdims=True), own_score)
        weight = jnp.exp(scores[...] - highest)
        scores[...] = weight
        own_weight = jnp.exp(own_score - highest)
        total = jnp.sum(weight, axis=0, keepdims=True) + own_weight
        factor = mix / total
        part = scores[...] * factor
        contrast[...] = (part - pltpu.roll(part, LANES // 2, 1)).astype(BF16)
        own_part = own_weight * factor
        own_contrast = own_part - pltpu.roll(own_part, LANES // 2, 1)
        pltpu.make_async_copy(vbuf.at[g], vbuf.at[g], v_sem.at[g]).wait()
        full = dot(contrast[...], vbuf[g], ((0,), (0,)))[: LANES // 2]
        own_rows = jnp.where(iota((GROUP, LANES), 0) == lane_seq, own_contrast, 0.0).astype(BF16)
        mixed = dot(own_rows, nvbuf[pl.ds(first, GROUP), :].astype(BF16), ((0,), (0,)))[: LANES // 2]
        out_seq = lax.rem(iota((LANES // 2, DV), 0), GROUP)
        for s in range(GROUP):
            mixed += jnp.where(out_seq == s, full[:, s * DV : (s + 1) * DV], 0.0)
        normal = mixed * row_scale(mixed) * hgain[...]
        for h in range(HEADS):
            heads[pl.ds(first, GROUP), h * DV : (h + 1) * DV] = normal[h * GROUP : (h + 1) * GROUP]

        @pl.when(g == 0)
        def _():
            for copy in own:
                copy.wait()
            for i, ref in enumerate((wg, wu, wd)):
                share(ref, i).start()

        return carry

    lax.fori_loop(0, GROUPS, attend, 0)

    wo_copy.wait()
    update = dot(heads[...].astype(BF16), wo[...])
    residual = (hidden[...].astype(F32) + update).astype(BF16)
    values = residual.astype(F32)
    resid[...] = values
    given = values * row_scale(values) * gain2[...]
    stacked = jnp.concatenate([given[:, c * WIDTH : (c + 1) * WIDTH] for c in range(PIECES)], axis=0).astype(BF16)
    packed = dot(pick, stacked).astype(BF16).reshape(CHIPS, ROWS, WIDTH)
    sendbuf[...] = packed
    recvbuf[0] = sendbuf[0]

    def dispatch(k, carry):
        pltpu.make_async_remote_copy(
            src_ref=sendbuf.at[k], dst_ref=recvbuf.at[k], send_sem=dsend_sem, recv_sem=drecv_sem.at[lax.div(k, PER)],
            device_id=(partner(k, 1),), device_id_type=MESH,
        ).start()
        return carry

    lax.fori_loop(1, CHIPS, dispatch, 0)

    for i, ref in enumerate((wg, wu, wd)):
        share(ref, i).wait()

    size = PER * ROWS
    line = iota((size, size), 0)
    column = iota((size, size), 1)

    def shuffled(a):
        return lax.rem(lax.div(a, CAP), PIECES) * (PER * CAP) + lax.div(a, ROWS) * CAP + lax.rem(a, CAP)

    to_pieces = (line == shuffled(column)).astype(BF16)
    to_messages = (shuffled(line) == column).astype(BF16)
    tall = PER * CAP

    def expert(b, carry):
        pieces = dot(to_pieces, recvbuf[pl.ds(b * PER, PER)].reshape(size, WIDTH)).astype(BF16)
        inner = []
        for j in range(2):
            gate = jnp.zeros((tall, PART), F32)
            upper = jnp.zeros((tall, PART), F32)
            for c in range(PIECES):
                flat = pieces[c * tall : (c + 1) * tall]
                gate += dot(flat, wg[j, c * WIDTH : (c + 1) * WIDTH, :])
                upper += dot(flat, wu[j, c * WIDTH : (c + 1) * WIDTH, :])
            inner.append((gate / (1.0 + jnp.exp(-gate)) * upper).astype(BF16))
        result = []
        for c in range(PIECES):
            cut = slice(c * WIDTH, (c + 1) * WIDTH)
            result.append((dot(inner[0], wd[0, :, cut]) + dot(inner[1], wd[1, :, cut])).astype(BF16))
        ybuf[pl.ds(b * PER, PER)] = dot(to_messages, jnp.concatenate(result, axis=0)).astype(BF16).reshape(PER, ROWS, WIDTH)

        def give(k, inside):
            pltpu.make_async_remote_copy(
                src_ref=ybuf.at[k], dst_ref=retbuf.at[k], send_sem=rsend_sem, recv_sem=rrecv_sem.at[b],
                device_id=(partner(k, -1),), device_id_type=MESH,
            ).start()
            return inside

        lax.fori_loop(jnp.maximum(b * PER, 1), (b + 1) * PER, give, 0)
        return carry

    def landed(ref, first, count, sem):
        part = ref.at[pl.ds(first, count)]
        pltpu.make_async_copy(part, part, sem).wait()

    landed(recvbuf, 1, PER - 1, drecv_sem.at[0])
    expert(0, 0)
    retbuf[0] = ybuf[0]

    def later(b, carry):
        landed(recvbuf, b * PER, PER, drecv_sem.at[b])
        return expert(b, carry)

    lax.fori_loop(1, BLOCKS, later, 0)

    total = jnp.zeros((2 * lanes, WIDTH), F32)
    for b in range(BLOCKS):
        if b == 0:
            landed(retbuf, 1, PER - 1, rrecv_sem.at[0])
        else:
            landed(retbuf, b * PER, PER, rrecv_sem.at[b])
        total += dot(wcomb[:, b * size : (b + 1) * size], retbuf[b * PER : (b + 1) * PER].reshape(size, WIDTH))
    routed = total[:lanes] + total[lanes:]
    for c in range(PIECES):
        cut = slice(c * WIDTH, (c + 1) * WIDTH)
        outbuf[:, cut] = (resid[:, cut] + routed[c * SEQS : (c + 1) * SEQS]).astype(BF16)
    out_copy = pltpu.make_async_copy(outbuf, out_h, out_sem.at[2])
    out_copy.start()
    landed(sendbuf, 1, CHIPS - 1, dsend_sem)
    landed(ybuf, 1, CHIPS - 1, rsend_sem)
    key_copy.wait()
    value_copy.wait()
    out_copy.wait()


def per_device(
    hidden, cache_keys, cache_values, lengths, first_gain, query_weight, key_weight, value_weight, mixing, head_gain,
    out_weight, second_gain, routes, route_weight, expert_gate, expert_up, expert_down,
):
    args = (
        hidden, cache_keys, cache_values, lengths, first_gain.reshape(1, D), query_weight, key_weight, value_weight,
        mixing, head_gain.reshape(1, DV), out_weight, second_gain.reshape(1, D), routes.T, route_weight.T,
        expert_gate, expert_up, expert_down,
    )
    vmem = pltpu.VMEM
    sem = pltpu.SemaphoreType.DMA
    scratch = [
        vmem((SEQS, D), BF16), vmem((GROUPS, SPAN, GROUP * 2 * DK), BF16), vmem((GROUPS, SPAN, GROUP * DV), BF16),
        pltpu.SMEM((SEQS,), jnp.int32), vmem((1, D), F32), vmem((D, HEADS * 2 * DK), BF16), vmem((D, 2 * DK), BF16),
        vmem((D, DV), BF16), pltpu.SMEM((HEADS,), F32), vmem((1, DV), F32), vmem((HEADS * DV, D), BF16),
        vmem((1, D), F32), vmem((TOP_K, SEQS), jnp.int32), vmem((TOP_K, SEQS), F32),
        vmem((2, D, PART), BF16), vmem((2, D, PART), BF16), vmem((2, PART, D), BF16),
        vmem((SEQS, HEADS * 2 * DK), F32), vmem((SEQS, 2 * DK), F32), vmem((SEQS, DV), F32),
        vmem((SPAN, LANES), F32), vmem((SPAN, LANES), BF16), vmem((SEQS, HEADS * DV), F32), vmem((SEQS, D), F32),
        vmem((SEQS, D), BF16), vmem((SEQS, 2 * DK), BF16), vmem((SEQS, DV), BF16),
        vmem((2 * PIECES * SEQS, CHIPS * ROWS), BF16),
        vmem((CHIPS, ROWS, WIDTH), BF16), vmem((CHIPS, ROWS, WIDTH), BF16),
        vmem((CHIPS, ROWS, WIDTH), BF16), vmem((CHIPS, ROWS, WIDTH), BF16),
        sem((10,)), sem((WCHUNKS,)), sem((GROUPS,)), sem((GROUPS,)), sem, sem((3,)), sem((3,)),
        sem((3,)), sem((3,)), sem, sem((BLOCKS,)), sem, sem((BLOCKS,)),
    ]
    return pl.pallas_call(
        kernel,
        out_shape=(
            jax.ShapeDtypeStruct((SEQS, D), BF16),
            jax.ShapeDtypeStruct((SEQS, 2 * DK), BF16),
            jax.ShapeDtypeStruct((SEQS, DV), BF16),
        ),
        in_specs=[pl.BlockSpec(memory_space=pl.ANY)] * len(args),
        out_specs=[pl.BlockSpec(memory_space=pl.ANY)] * 3,
        scratch_shapes=scratch,
        compiler_params=pltpu.CompilerParams(
            collective_id=0, has_side_effects=True, vmem_limit_bytes=60 * 1024 * 1024
        ),
        name="layer",
    )(*args)


def solution(mesh):
    return jax.shard_map(
        per_device,
        mesh=mesh,
        in_specs=(
            P("ep", None), P("ep", None, None), P("ep", None, None), P("ep"), P(), P(), P(), P(), P(), P(), P(), P(),
            P("ep", None), P("ep", None), P("ep", None, None), P("ep", None, None), P("ep", None, None),
        ),
        out_specs=(P("ep", None), P("ep", None), P("ep", None)),
        check_vma=False,
    )
```

```python
import functools

import jax
import jax.numpy as jnp
from jax import lax
from jax.experimental import pallas as pl
from jax.experimental.pallas import tpu as pltpu
from jax.sharding import PartitionSpec as P

MESH = pl.DeviceIdType.MESH
BF16 = jnp.bfloat16
F32 = jnp.float32

D = 2048
HEADS = 8
DK = 64
DV = 128
PART = 256
TOP_K = 4
SEQS = 32
SPAN = 1024
CAP = 4
CHIPS = 64
SIDE = 4
GROUP = 8
GROUPS = SEQS // GROUP
WCHUNKS = 4
PIECES = 2
WIDTH = D // PIECES
ROWS = CAP * PIECES
BLOCKS = 4
PER = CHIPS // BLOCKS
MUL = 37
INV = pow(MUL, -1, CHIPS)
LANES = GROUP * HEADS * 2
EPS = 1e-06


def dot(a, b, dims=((1,), (0,))):
    return lax.dot_general(a, b, (dims, ((), ())), preferred_element_type=F32)


def iota(shape, axis):
    return lax.broadcasted_iota(jnp.int32, shape, axis)


def row_scale(values):
    return lax.rsqrt(jnp.mean(values * values, axis=-1, keepdims=True) + EPS)


def kernel(
    hidden_h, keys_h, values_h, lengths_h, gain1_h, wq_h, wk_h, wv_h, mixing_h, hgain_h, wo_h, gain2_h,
    routes_h, rweight_h, gate_h, up_h, down_h,
    out,
    hidden, kbuf, vbuf, lens, gain1, wq, wk, wv, mixing, hgain, wo, gain2, routes, rweight, wg, wu, wd,
    qbuf, nkbuf, nvbuf, scores, contrast, heads, resid, picked,
    wcomb, sendbuf, recvbuf, ybuf, retbuf,
    small_sem, wq_sem, k_sem, v_sem, wo_sem, exp_sem,
    wsend_sem, wrecv_sem, dsend_sem, drecv_sem, rsend_sem, rrecv_sem,
):
    me = lax.axis_index("ep")
    core = lax.rem(me, 2)
    chip = lax.div(me, 2)
    cx = lax.rem(chip, SIDE)
    cy = lax.rem(lax.div(chip, SIDE), SIDE)
    cz = lax.div(chip, SIDE * SIDE)
    sibling = chip * 2 + (1 - core)

    ahead_x = [lax.rem(cx + d, SIDE) * 2 + core for d in range(SIDE)]
    ahead_y = [lax.rem(cy + d, SIDE) * (SIDE * 2) for d in range(SIDE)]
    ahead_z = [lax.rem(cz + d, SIDE) * (SIDE * SIDE * 2) for d in range(SIDE)]

    def partner(k, sign):
        rel = k * INV % CHIPS
        dx, dy, dz = rel % SIDE, rel // SIDE % SIDE, rel // (SIDE * SIDE)
        return ahead_z[sign * dz % SIDE] + ahead_y[sign * dy % SIDE] + ahead_x[sign * dx % SIDE]

    smalls = [
        (routes_h, routes), (rweight_h, rweight), (hidden_h, hidden), (gain1_h, gain1), (lengths_h, lens),
        (mixing_h, mixing), (hgain_h, hgain), (gain2_h, gain2), (wk_h, wk), (wv_h, wv),
    ]
    small = [pltpu.make_async_copy(a, b, small_sem.at[i]) for i, (a, b) in enumerate(smalls)]
    for copy in small:
        copy.start()
    step = D // WCHUNKS
    wq_copies = [
        pltpu.make_async_copy(wq_h.at[pl.ds(i * step, step)], wq.at[pl.ds(i * step, step)], wq_sem.at[i])
        for i in range(WCHUNKS)
    ]
    for copy in wq_copies:
        copy.start()

    def fetch(g, carry):
        for s in range(GROUP):
            pltpu.make_async_copy(keys_h.at[g * GROUP + s], kbuf.at[g, :, pl.ds(s * 2 * DK, 2 * DK)], k_sem.at[g]).start()
        for s in range(GROUP):
            pltpu.make_async_copy(values_h.at[g * GROUP + s], vbuf.at[g, :, pl.ds(s * DV, DV)], v_sem.at[g]).start()
        return carry

    own = [
        pltpu.make_async_copy(gate_h.at[0], wg.at[core], exp_sem.at[0]),
        pltpu.make_async_copy(up_h.at[0], wu.at[core], exp_sem.at[1]),
        pltpu.make_async_copy(down_h.at[0], wd.at[core], exp_sem.at[2]),
    ]
    wo_copy = pltpu.make_async_copy(wo_h, wo, wo_sem)
    lax.fori_loop(0, GROUPS - 1, fetch, 0)
    wo_copy.start()
    fetch(GROUPS - 1, 0)
    for copy in own:
        copy.start()

    barrier = pltpu.get_barrier_semaphore()
    for k in range(1, CHIPS):
        pl.semaphore_signal(barrier, inc=1, device_id=(partner(k, 1),), device_id_type=MESH)
    pl.semaphore_signal(barrier, inc=1, device_id=(sibling,), device_id_type=MESH)

    lanes = PIECES * SEQS
    small[0].wait()
    small[1].wait()
    spread = (iota((SEQS, lanes), 0) == lax.rem(iota((SEQS, lanes), 1), SEQS)).astype(BF16)
    picks = dot(routes[...].astype(F32).astype(BF16), spread).astype(jnp.int32)
    lowest = jnp.min(picks, axis=0, keepdims=True)
    named = (iota((CHIPS, lanes), 0) == lowest).astype(F32)
    earlier = (iota((lanes, lanes), 0) < lax.rem(iota((lanes, lanes), 1), SEQS)).astype(F32)
    before = dot(named.astype(BF16), earlier.astype(BF16))
    place = jnp.sum(before * named, axis=0, keepdims=True).astype(jnp.int32)
    ex = lax.rem(picks, SIDE)
    ey = lax.rem(lax.div(picks, SIDE), SIDE)
    ez = lax.div(picks, SIDE * SIDE)
    offset = (
        lax.rem(ez - cz + SIDE, SIDE) * (SIDE * SIDE) + lax.rem(ey - cy + SIDE, SIDE) * SIDE + lax.rem(ex - cx + SIDE, SIDE)
    )
    piece = lax.div(iota((1, lanes), 1), SEQS)
    target = lax.rem(offset * MUL, CHIPS) * ROWS + piece * CAP + place
    high = rweight[...].astype(BF16)
    low = (rweight[...] - high.astype(F32)).astype(BF16)
    high = dot(high, spread)
    low = dot(low, spread)
    slot = iota((CHIPS * ROWS, lanes), 0)
    pick = jnp.zeros((CHIPS * ROWS, lanes), F32)
    comb_high = jnp.zeros((CHIPS * ROWS, lanes), F32)
    comb_low = jnp.zeros((CHIPS * ROWS, lanes), F32)
    for k in range(TOP_K):
        hit = slot == target[k : k + 1, :]
        pick = jnp.where(hit, 1.0, pick)
        comb_high = jnp.where(hit, high[k : k + 1, :], comb_high)
        comb_low = jnp.where(hit, low[k : k + 1, :], comb_low)
    picked[...] = pick.astype(BF16)
    wcomb[...] = jnp.transpose(jnp.concatenate([comb_high, comb_low], axis=1)).astype(BF16)

    small[2].wait()
    small[3].wait()
    values = hidden[...].astype(F32)
    normed = (values * row_scale(values) * gain1[...]).astype(BF16)
    query = jnp.zeros((SEQS, HEADS * 2 * DK), F32)
    for i in range(WCHUNKS):
        wq_copies[i].wait()
        query += dot(normed[:, i * step : (i + 1) * step], wq[i * step : (i + 1) * step, :])
    qbuf[...] = query.astype(BF16).astype(F32) * DK ** (-0.5)
    for copy in small[4:]:
        copy.wait()
    new_key = dot(normed, wk[...]).astype(BF16)
    new_value = dot(normed, wv[...]).astype(BF16)
    out[:, D : D + 2 * DK] = new_key
    out[:, D + 2 * DK :] = new_value
    nkbuf[...] = new_key.astype(F32)
    nvbuf[...] = new_value.astype(F32)

    def share(source, index):
        return pltpu.make_async_remote_copy(
            src_ref=source.at[core], dst_ref=source.at[core], send_sem=wsend_sem.at[index],
            recv_sem=wrecv_sem.at[index], device_id=(sibling,), device_id_type=MESH,
        )

    lane = iota((1, LANES), 1)
    lane_seq = lax.rem(lane, GROUP)
    lane_head = lax.rem(lax.div(lane, GROUP), HEADS)
    mix = jnp.zeros((1, LANES), F32)
    for h in range(HEADS):
        mix = jnp.where(lane_head == h, mixing[h], mix)
    mix = jnp.where(lane < LANES // 2, 1.0, mix)
    row = iota((LANES, 2 * DK), 0)
    col = iota((LANES, 2 * DK), 1)
    same_map = lax.div(row, LANES // 2) == lax.div(col, DK)
    row_seq = lax.rem(row, GROUP)

    def attend(g, carry):
        first = pl.multiple_of(g * GROUP, GROUP)
        rows = [qbuf[pl.ds(first, GROUP), h * 2 * DK : (h + 1) * 2 * DK] for h in range(HEADS)]
        block = jnp.concatenate(rows + rows, axis=0)
        block = jnp.where(same_map, block, 0.0)
        diag = jnp.concatenate(
            [jnp.where(row_seq == s, block, 0.0).astype(BF16) for s in range(GROUP)], axis=1
        )
        limit = jnp.zeros((1, LANES), jnp.int32)
        for s in range(GROUP):
            limit = jnp.where(lane_seq == s, lens[g * GROUP + s], limit)
        fresh = nkbuf[pl.ds(first, GROUP), :]
        fresh_rows = jnp.concatenate(
            [jnp.where(iota((GROUP, 2 * DK), 0) == s, fresh, 0.0).astype(BF16) for s in range(GROUP)], axis=1
        )
        own_score = jnp.sum(dot(fresh_rows, diag, ((1,), (1,))), axis=0, keepdims=True)
        pltpu.make_async_copy(kbuf.at[g], kbuf.at[g], k_sem.at[g]).wait()
        score = dot(kbuf[g], diag, ((1,), (1,)))
        score = jnp.where(iota((SPAN, LANES), 0) < limit, score, -jnp.inf)
        scores[...] = score
        highest = jnp.maximum(jnp.max(score, axis=0, keepdims=True), own_score)
        weight = jnp.exp(scores[...] - highest)
        scores[...] = weight
        own_weight = jnp.exp(own_score - highest)
        total = jnp.sum(weight, axis=0, keepdims=True) + own_weight
        factor = mix / total
        part = scores[...] * factor
        contrast[...] = (part - pltpu.roll(part, LANES // 2, 1)).astype(BF16)
        own_part = own_weight * factor
        own_contrast = own_part - pltpu.roll(own_part, LANES // 2, 1)
        pltpu.make_async_copy(vbuf.at[g], vbuf.at[g], v_sem.at[g]).wait()
        full = dot(contrast[...], vbuf[g], ((0,), (0,)))[: LANES // 2]
        own_rows = jnp.where(iota((GROUP, LANES), 0) == lane_seq, own_contrast, 0.0).astype(BF16)
        mixed = dot(own_rows, nvbuf[pl.ds(first, GROUP), :].astype(BF16), ((0,), (0,)))[: LANES // 2]
        out_seq = lax.rem(iota((LANES // 2, DV), 0), GROUP)
        for s in range(GROUP):
            mixed += jnp.where(out_seq == s, full[:, s * DV : (s + 1) * DV], 0.0)
        normal = mixed * row_scale(mixed) * hgain[...]
        for h in range(HEADS):
            heads[pl.ds(first, GROUP), h * DV : (h + 1) * DV] = normal[h * GROUP : (h + 1) * GROUP]
        return carry

    lax.fori_loop(0, GROUPS, attend, 0)

    wo_copy.wait()
    update = dot(heads[...].astype(BF16), wo[...])
    residual = (hidden[...].astype(F32) + update).astype(BF16)
    values = residual.astype(F32)
    resid[...] = values
    given = values * row_scale(values) * gain2[...]
    stacked = jnp.concatenate([given[:, c * WIDTH : (c + 1) * WIDTH] for c in range(PIECES)], axis=0).astype(BF16)
    packed = dot(picked[...], stacked).astype(BF16).reshape(CHIPS, ROWS, WIDTH)
    sendbuf[...] = packed

    pl.semaphore_wait(barrier, CHIPS)
    for k in range(1, CHIPS):
        pltpu.make_async_remote_copy(
            src_ref=sendbuf.at[k], dst_ref=recvbuf.at[k], send_sem=dsend_sem, recv_sem=drecv_sem.at[k // PER],
            device_id=(partner(k, 1),), device_id_type=MESH,
        ).start()
    for copy in own:
        copy.wait()
    for i, ref in enumerate((wg, wu, wd)):
        share(ref, i).start()
    recvbuf[0] = sendbuf[0]

    size = PER * ROWS
    line = iota((size, size), 0)
    column = iota((size, size), 1)

    def shuffled(a):
        return lax.rem(lax.div(a, CAP), PIECES) * (PER * CAP) + lax.div(a, ROWS) * CAP + lax.rem(a, CAP)

    to_pieces = (line == shuffled(column)).astype(BF16)
    to_messages = (shuffled(line) == column).astype(BF16)
    tall = PER * CAP

    def expert(b):
        pieces = dot(to_pieces, recvbuf[pl.ds(b * PER, PER)].reshape(size, WIDTH)).astype(BF16)
        inner = []
        for j in range(2):
            gate = jnp.zeros((tall, PART), F32)
            upper = jnp.zeros((tall, PART), F32)
            for c in range(PIECES):
                flat = pieces[c * tall : (c + 1) * tall]
                gate += dot(flat, wg[j, c * WIDTH : (c + 1) * WIDTH, :])
                upper += dot(flat, wu[j, c * WIDTH : (c + 1) * WIDTH, :])
            inner.append((gate / (1.0 + jnp.exp(-gate)) * upper).astype(BF16))
        result = []
        for c in range(PIECES):
            cut = slice(c * WIDTH, (c + 1) * WIDTH)
            result.append((dot(inner[0], wd[0, :, cut]) + dot(inner[1], wd[1, :, cut])).astype(BF16))
        ybuf[pl.ds(b * PER, PER)] = dot(to_messages, jnp.concatenate(result, axis=0)).astype(BF16).reshape(PER, ROWS, WIDTH)
        for k in range(max(b * PER, 1), (b + 1) * PER):
            pltpu.make_async_remote_copy(
                src_ref=ybuf.at[k], dst_ref=retbuf.at[k], send_sem=rsend_sem, recv_sem=rrecv_sem.at[b],
                device_id=(partner(k, -1),), device_id_type=MESH,
            ).start()

    def landed(ref, first, count, sem):
        part = ref.at[pl.ds(first, count)]
        pltpu.make_async_copy(part, part, sem).wait()

    def wait_block(ref, b, sem):
        landed(ref, max(b * PER, 1), PER - (b == 0), sem.at[b])

    for b in range(BLOCKS):
        wait_block(recvbuf, b, drecv_sem)
        if b == 0:
            for i, ref in enumerate((wg, wu, wd)):
                share(ref, i).wait()
        expert(b)
    retbuf[0] = ybuf[0]

    total = jnp.zeros((2 * lanes, WIDTH), F32)
    for b in range(BLOCKS):
        wait_block(retbuf, b, rrecv_sem)
        total += dot(wcomb[:, b * size : (b + 1) * size], retbuf[b * PER : (b + 1) * PER].reshape(size, WIDTH))
    routed = total[:lanes] + total[lanes:]
    for c in range(PIECES):
        cut = slice(c * WIDTH, (c + 1) * WIDTH)
        out[:, cut] = (resid[:, cut] + routed[c * SEQS : (c + 1) * SEQS]).astype(BF16)
    landed(sendbuf, 1, CHIPS - 1, dsend_sem)
    landed(ybuf, 1, CHIPS - 1, rsend_sem)


def finish(packed, out, new_key, new_value, sem):
    copies = [
        pltpu.make_async_copy(packed.at[:, pl.ds(0, D)], out, sem.at[0]),
        pltpu.make_async_copy(packed.at[:, pl.ds(D, 2 * DK)], new_key, sem.at[1]),
        pltpu.make_async_copy(packed.at[:, pl.ds(D + 2 * DK, DV)], new_value, sem.at[2]),
    ]
    for copy in copies:
        copy.start()
    for copy in copies:
        copy.wait()


def per_device(
    hidden, cache_keys, cache_values, lengths, first_gain, query_weight, key_weight, value_weight, mixing, head_gain,
    out_weight, second_gain, routes, route_weight, expert_gate, expert_up, expert_down,
):
    args = (
        hidden, cache_keys, cache_values, lengths, first_gain.reshape(1, D), query_weight, key_weight, value_weight,
        mixing, head_gain.reshape(1, DV), out_weight, second_gain.reshape(1, D), routes.T, route_weight.T,
        expert_gate, expert_up, expert_down,
    )
    vmem = pltpu.VMEM
    sem = pltpu.SemaphoreType.DMA
    scratch = [
        vmem((SEQS, D), BF16), vmem((GROUPS, SPAN, GROUP * 2 * DK), BF16), vmem((GROUPS, SPAN, GROUP * DV), BF16),
        pltpu.SMEM((SEQS,), jnp.int32), vmem((1, D), F32), vmem((D, HEADS * 2 * DK), BF16), vmem((D, 2 * DK), BF16),
        vmem((D, DV), BF16), pltpu.SMEM((HEADS,), F32), vmem((1, DV), F32), vmem((HEADS * DV, D), BF16),
        vmem((1, D), F32), vmem((TOP_K, SEQS), jnp.int32), vmem((TOP_K, SEQS), F32),
        vmem((2, D, PART), BF16), vmem((2, D, PART), BF16), vmem((2, PART, D), BF16),
        vmem((SEQS, HEADS * 2 * DK), F32), vmem((SEQS, 2 * DK), F32), vmem((SEQS, DV), F32),
        vmem((SPAN, LANES), F32), vmem((SPAN, LANES), BF16), vmem((SEQS, HEADS * DV), F32), vmem((SEQS, D), F32),
        vmem((CHIPS * ROWS, PIECES * SEQS), BF16),
        vmem((2 * PIECES * SEQS, CHIPS * ROWS), BF16),
        vmem((CHIPS, ROWS, WIDTH), BF16), vmem((CHIPS, ROWS, WIDTH), BF16),
        vmem((CHIPS, ROWS, WIDTH), BF16), vmem((CHIPS, ROWS, WIDTH), BF16),
        sem((10,)), sem((WCHUNKS,)), sem((GROUPS,)), sem((GROUPS,)), sem, sem((3,)),
        sem((3,)), sem((3,)), sem, sem((BLOCKS,)), sem, sem((BLOCKS,)),
    ]
    packed = pl.pallas_call(
        kernel,
        out_shape=pltpu.VMEM((SEQS, D + 2 * DK + DV), BF16),
        in_specs=[pl.BlockSpec(memory_space=pltpu.HBM)] * len(args),
        out_specs=pl.BlockSpec(memory_space=pltpu.VMEM),
        scratch_shapes=scratch,
        compiler_params=pltpu.CompilerParams(
            collective_id=0, has_side_effects=True, vmem_limit_bytes=62 * 1024 * 1024
        ),
        name="layer",
    )(*args)
    return pl.pallas_call(
        finish,
        out_shape=(
            jax.ShapeDtypeStruct((SEQS, D), BF16),
            jax.ShapeDtypeStruct((SEQS, 2 * DK), BF16),
            jax.ShapeDtypeStruct((SEQS, DV), BF16),
        ),
        in_specs=[pl.BlockSpec(memory_space=pltpu.VMEM)],
        out_specs=[pl.BlockSpec(memory_space=pltpu.HBM)] * 3,
        scratch_shapes=[sem((3,))],
        compiler_params=pltpu.CompilerParams(vmem_limit_bytes=8 * 1024 * 1024),
        name="finish",
    )(packed)


def solution(mesh):
    return jax.shard_map(
        per_device,
        mesh=mesh,
        in_specs=(
            P("ep", None), P("ep", None, None), P("ep", None, None), P("ep"), P(), P(), P(), P(), P(), P(), P(), P(),
            P("ep", None), P("ep", None), P("ep", None, None), P("ep", None, None), P("ep", None, None),
        ),
        out_specs=(P("ep", None), P("ep", None), P("ep", None)),
        check_vma=False,
    )
```

```python
import functools

import jax
import jax.numpy as jnp
from jax import lax
from jax.experimental import pallas as pl
from jax.experimental.pallas import tpu as pltpu
from jax.sharding import PartitionSpec as P

MESH = pl.DeviceIdType.MESH
BF16 = jnp.bfloat16
F32 = jnp.float32

D = 2048
HEADS = 8
DK = 64
DV = 128
PART = 256
TOP_K = 4
SEQS = 32
SPAN = 1024
CAP = 4
CHIPS = 64
SIDE = 4
GROUP = 16
GROUPS = SEQS // GROUP
WCHUNKS = 4
PIECES = 2
WIDTH = D // PIECES
ROWS = CAP * PIECES
BLOCKS = 4
PER = CHIPS // BLOCKS
MUL = 45
INV = pow(MUL, -1, CHIPS)
LANES = GROUP * HEADS
CUT = 128
EPS = 1e-06


def dot(a, b, dims=((1,), (0,))):
    return lax.dot_general(a, b, (dims, ((), ())), preferred_element_type=F32)


def iota(shape, axis):
    return lax.broadcasted_iota(jnp.int32, shape, axis)


def row_scale(values):
    return lax.rsqrt(jnp.mean(values * values, axis=-1, keepdims=True) + EPS)


def kernel(
    hidden_h, keys_h, values_h, lengths_h, gain1_h, wq_h, wk_h, wv_h, mixing_h, hgain_h, wo_h, gain2_h,
    routes_h, rweight_h, gate_h, up_h, down_h,
    out,
    hidden, kbuf, vbuf, lens, gain1, wq, wk, wv, mixing, hgain, wo, gain2, routes, rweight, wg, wu, wd,
    qbuf, nkbuf, nvbuf, diag, scores, contrast, heads, resid, picked,
    wcomb, sendbuf, recvbuf, ybuf, retbuf,
    small_sem, wq_sem, k_sem, v_sem, wo_sem, exp_sem,
    wsend_sem, wrecv_sem, dsend_sem, drecv_sem, rsend_sem, rrecv_sem,
):
    me = lax.axis_index("ep")
    core = lax.rem(me, 2)
    chip = lax.div(me, 2)
    cx = lax.rem(chip, SIDE)
    cy = lax.rem(lax.div(chip, SIDE), SIDE)
    cz = lax.div(chip, SIDE * SIDE)
    sibling = chip * 2 + (1 - core)

    ahead_x = [lax.rem(cx + d, SIDE) * 2 + core for d in range(SIDE)]
    ahead_y = [lax.rem(cy + d, SIDE) * (SIDE * 2) for d in range(SIDE)]
    ahead_z = [lax.rem(cz + d, SIDE) * (SIDE * SIDE * 2) for d in range(SIDE)]

    def partner(k, sign):
        rel = k * INV % CHIPS
        dx, dy, dz = rel % SIDE, rel // SIDE % SIDE, rel // (SIDE * SIDE)
        return ahead_z[sign * dz % SIDE] + ahead_y[sign * dy % SIDE] + ahead_x[sign * dx % SIDE]

    smalls = [
        (routes_h, routes), (rweight_h, rweight), (hidden_h, hidden), (gain1_h, gain1), (lengths_h, lens),
        (mixing_h, mixing), (hgain_h, hgain), (gain2_h, gain2), (wk_h, wk), (wv_h, wv),
    ]
    small = [pltpu.make_async_copy(a, b, small_sem.at[i]) for i, (a, b) in enumerate(smalls)]
    for copy in small:
        copy.start()
    step = D // WCHUNKS
    wq_copies = [
        pltpu.make_async_copy(wq_h.at[pl.ds(i * step, step)], wq.at[pl.ds(i * step, step)], wq_sem.at[i])
        for i in range(WCHUNKS)
    ]
    for copy in wq_copies:
        copy.start()

    def fetch_keys(g):
        part = pl.ds(g * GROUP, GROUP)
        pltpu.make_async_copy(keys_h.at[part], kbuf.at[part], k_sem.at[g]).start()

    def fetch_values(g):
        part = pl.ds(g * GROUP, GROUP)
        pltpu.make_async_copy(values_h.at[part], vbuf.at[part], v_sem.at[g]).start()

    own = [
        pltpu.make_async_copy(gate_h.at[0], wg.at[core], exp_sem.at[0]),
        pltpu.make_async_copy(up_h.at[0], wu.at[core], exp_sem.at[1]),
        pltpu.make_async_copy(down_h.at[0], wd.at[core], exp_sem.at[2]),
    ]
    wo_copy = pltpu.make_async_copy(wo_h, wo, wo_sem)

    def fetch_own():
        for copy in own:
            copy.start()

    barrier = pltpu.get_barrier_semaphore()
    for k in range(1, CHIPS):
        pl.semaphore_signal(barrier, inc=1, device_id=(partner(k, 1),), device_id_type=MESH)
    pl.semaphore_signal(barrier, inc=1, device_id=(sibling,), device_id_type=MESH)

    lanes = PIECES * SEQS
    small[0].wait()
    small[1].wait()
    spread = (iota((SEQS, lanes), 0) == lax.rem(iota((SEQS, lanes), 1), SEQS)).astype(BF16)
    picks = dot(routes[...].astype(F32).astype(BF16), spread).astype(jnp.int32)
    lowest = jnp.min(picks, axis=0, keepdims=True)
    named = (iota((CHIPS, lanes), 0) == lowest).astype(F32)
    earlier = (iota((lanes, lanes), 0) < lax.rem(iota((lanes, lanes), 1), SEQS)).astype(F32)
    before = dot(named.astype(BF16), earlier.astype(BF16))
    place = jnp.sum(before * named, axis=0, keepdims=True).astype(jnp.int32)
    ex = lax.rem(picks, SIDE)
    ey = lax.rem(lax.div(picks, SIDE), SIDE)
    ez = lax.div(picks, SIDE * SIDE)
    offset = (
        lax.rem(ez - cz + SIDE, SIDE) * (SIDE * SIDE) + lax.rem(ey - cy + SIDE, SIDE) * SIDE + lax.rem(ex - cx + SIDE, SIDE)
    )
    piece = lax.div(iota((1, lanes), 1), SEQS)
    target = lax.rem(offset * MUL, CHIPS) * ROWS + piece * CAP + place
    high = rweight[...].astype(BF16)
    low = (rweight[...] - high.astype(F32)).astype(BF16)
    high = dot(high, spread)
    low = dot(low, spread)
    slot = iota((CHIPS * ROWS, lanes), 0)
    pick = jnp.zeros((CHIPS * ROWS, lanes), F32)
    comb_high = jnp.zeros((CHIPS * ROWS, lanes), F32)
    comb_low = jnp.zeros((CHIPS * ROWS, lanes), F32)
    for k in range(TOP_K):
        hit = slot == target[k : k + 1, :]
        pick = jnp.where(hit, 1.0, pick)
        comb_high = jnp.where(hit, high[k : k + 1, :], comb_high)
        comb_low = jnp.where(hit, low[k : k + 1, :], comb_low)
    picked[...] = pick.astype(BF16)
    wcomb[...] = jnp.transpose(jnp.concatenate([comb_high, comb_low], axis=1)).astype(BF16)

    fetch_keys(0)
    small[2].wait()
    small[3].wait()
    values = hidden[...].astype(F32)
    normed = (values * row_scale(values) * gain1[...]).astype(BF16)
    query = jnp.zeros((SEQS, HEADS * 2 * DK), F32)
    for i in range(WCHUNKS):
        wq_copies[i].wait()
        query += dot(normed[:, i * step : (i + 1) * step], wq[i * step : (i + 1) * step, :])
    qbuf[...] = query.astype(BF16).astype(F32) * DK ** (-0.5)
    for copy in small[4:]:
        copy.wait()
    new_key = dot(normed, wk[...]).astype(BF16)
    new_value = dot(normed, wv[...]).astype(BF16)
    out[:, D : D + 2 * DK] = new_key
    out[:, D + 2 * DK :] = new_value
    nkbuf[...] = new_key.astype(F32)
    nvbuf[...] = new_value.astype(F32)

    fetch_values(0)

    def share(source, index):
        return pltpu.make_async_remote_copy(
            src_ref=source.at[core], dst_ref=source.at[core], send_sem=wsend_sem.at[index],
            recv_sem=wrecv_sem.at[index], device_id=(sibling,), device_id_type=MESH,
        )

    lane = iota((1, LANES), 1)
    lane_seq = lax.rem(lane, GROUP)
    mix = jnp.zeros((1, LANES), F32)
    for h in range(HEADS):
        mix = jnp.where(lax.div(lane, GROUP) == h, mixing[h], mix)
    row_seq = lax.rem(iota((LANES, DV), 0), GROUP)
    blank = jnp.zeros((DK, LANES), BF16)

    def attend(g, with_keys, with_values):
        first = g * GROUP
        block = jnp.concatenate(
            [qbuf[pl.ds(first, GROUP), h * 2 * DK : (h + 1) * 2 * DK] for h in range(HEADS)], axis=0
        ).T
        fresh = jnp.concatenate([nkbuf[pl.ds(first, GROUP), :]] * HEADS, axis=0).T
        limit = jnp.zeros((1, LANES), jnp.int32)
        for s in range(GROUP):
            limit = jnp.where(lane_seq == s, lens[g * GROUP + s], limit)
            one = jnp.where(lane_seq == s, block, 0.0).astype(BF16)
            for m in range(2):
                for half in range(2):
                    diag[s * 2 * DK + half * DK : s * 2 * DK + (half + 1) * DK, m * LANES : (m + 1) * LANES] = (
                        one[half * DK : (half + 1) * DK] if half == m else blank
                    )
        both = block * fresh
        own_score = jnp.concatenate(
            [jnp.sum(both[m * DK : (m + 1) * DK], axis=0, keepdims=True) for m in range(2)], axis=1
        )
        limit = jnp.concatenate([limit, limit], axis=1)
        pltpu.make_async_copy(keys_h.at[pl.ds(first, GROUP)], kbuf.at[pl.ds(first, GROUP)], k_sem.at[g]).wait()
        with_keys()
        score = jnp.zeros((SPAN, 2 * LANES), F32)
        for s in range(0, GROUP, 2):
            pair = jnp.concatenate([kbuf[first + s], kbuf[first + s + 1]], axis=1)
            score += dot(pair, diag[s * 2 * DK : (s + 2) * 2 * DK])
        score = jnp.where(iota((SPAN, 2 * LANES), 0) < limit, score, -jnp.inf)
        scores[...] = score
        highest = jnp.maximum(jnp.max(score, axis=0, keepdims=True), own_score)
        own_weight = jnp.exp(own_score - highest)
        total = own_weight
        for c in range(0, SPAN, CUT):
            weight = jnp.exp(scores[c : c + CUT] - highest)
            scores[c : c + CUT] = weight
            total += jnp.sum(weight, axis=0, keepdims=True)
        factor = jnp.concatenate([jnp.ones((1, LANES), F32), mix], axis=1) / total
        for c in range(0, SPAN, CUT):
            part = scores[c : c + CUT] * factor
            contrast[:, c : c + CUT] = (part[:, :LANES] - part[:, LANES:]).T.astype(BF16)
        own_part = own_weight * factor
        own_contrast = (own_part[:, :LANES] - own_part[:, LANES:]).astype(BF16).astype(F32)
        own_rows = jnp.broadcast_to(own_contrast, (DV, LANES)).T
        mixed = own_rows * jnp.concatenate([nvbuf[pl.ds(first, GROUP), :]] * HEADS, axis=0)
        pltpu.make_async_copy(values_h.at[pl.ds(first, GROUP)], vbuf.at[pl.ds(first, GROUP)], v_sem.at[g]).wait()
        with_values()
        for s in range(0, GROUP, 2):
            pair = dot(contrast[...], jnp.concatenate([vbuf[first + s], vbuf[first + s + 1]], axis=1))
            mixed += jnp.where(row_seq == s, pair[:, :DV], 0.0) + jnp.where(row_seq == s + 1, pair[:, DV:], 0.0)
        normal = mixed * row_scale(mixed) * hgain[...]
        for h in range(HEADS):
            heads[pl.ds(first, GROUP), h * DV : (h + 1) * DV] = normal[h * GROUP : (h + 1) * GROUP]

    def with_first_keys():
        fetch_own()
        fetch_keys(1)

    attend(0, with_first_keys, functools.partial(fetch_values, 1))
    pl.semaphore_wait(barrier, CHIPS)
    for copy in own:
        copy.wait()
    for i, ref in enumerate((wg, wu, wd)):
        share(ref, i).start()
    attend(1, wo_copy.start, lambda: None)

    wo_copy.wait()
    update = dot(heads[...].astype(BF16), wo[...])
    residual = (hidden[...].astype(F32) + update).astype(BF16)
    values = residual.astype(F32)
    resid[...] = values
    given = values * row_scale(values) * gain2[...]
    stacked = jnp.concatenate([given[:, c * WIDTH : (c + 1) * WIDTH] for c in range(PIECES)], axis=0).astype(BF16)
    packed = dot(picked[...], stacked).astype(BF16).reshape(CHIPS, ROWS, WIDTH)
    sendbuf[...] = packed

    for k in range(1, CHIPS):
        pltpu.make_async_remote_copy(
            src_ref=sendbuf.at[k], dst_ref=recvbuf.at[k], send_sem=dsend_sem, recv_sem=drecv_sem.at[k // PER],
            device_id=(partner(k, 1),), device_id_type=MESH,
        ).start()
    recvbuf[0] = sendbuf[0]

    size = PER * ROWS
    line = iota((size, size), 0)
    column = iota((size, size), 1)

    def shuffled(a):
        return lax.rem(lax.div(a, CAP), PIECES) * (PER * CAP) + lax.div(a, ROWS) * CAP + lax.rem(a, CAP)

    to_pieces = (line == shuffled(column)).astype(BF16)
    to_messages = (shuffled(line) == column).astype(BF16)
    tall = PER * CAP

    def expert(b):
        pieces = dot(to_pieces, recvbuf[pl.ds(b * PER, PER)].reshape(size, WIDTH)).astype(BF16)
        inner = []
        for j in range(2):
            gate = jnp.zeros((tall, PART), F32)
            upper = jnp.zeros((tall, PART), F32)
            for c in range(PIECES):
                flat = pieces[c * tall : (c + 1) * tall]
                gate += dot(flat, wg[j, c * WIDTH : (c + 1) * WIDTH, :])
                upper += dot(flat, wu[j, c * WIDTH : (c + 1) * WIDTH, :])
            inner.append((gate / (1.0 + jnp.exp(-gate)) * upper).astype(BF16))
        result = []
        for c in range(PIECES):
            cut = slice(c * WIDTH, (c + 1) * WIDTH)
            result.append((dot(inner[0], wd[0, :, cut]) + dot(inner[1], wd[1, :, cut])).astype(BF16))
        ybuf[pl.ds(b * PER, PER)] = dot(to_messages, jnp.concatenate(result, axis=0)).astype(BF16).reshape(PER, ROWS, WIDTH)
        for k in range(max(b * PER, 1), (b + 1) * PER):
            pltpu.make_async_remote_copy(
                src_ref=ybuf.at[k], dst_ref=retbuf.at[k], send_sem=rsend_sem, recv_sem=rrecv_sem.at[b],
                device_id=(partner(k, -1),), device_id_type=MESH,
            ).start()

    def landed(ref, first, count, sem):
        part = ref.at[pl.ds(first, count)]
        pltpu.make_async_copy(part, part, sem).wait()

    def wait_block(ref, b, sem):
        landed(ref, max(b * PER, 1), PER - (b == 0), sem.at[b])

    for b in range(BLOCKS):
        wait_block(recvbuf, b, drecv_sem)
        if b == 0:
            for i, ref in enumerate((wg, wu, wd)):
                share(ref, i).wait()
        expert(b)
    retbuf[0] = ybuf[0]

    total = jnp.zeros((2 * lanes, WIDTH), F32)
    for b in range(BLOCKS):
        wait_block(retbuf, b, rrecv_sem)
        total += dot(wcomb[:, b * size : (b + 1) * size], retbuf[b * PER : (b + 1) * PER].reshape(size, WIDTH))
    routed = total[:lanes] + total[lanes:]
    for c in range(PIECES):
        cut = slice(c * WIDTH, (c + 1) * WIDTH)
        out[:, cut] = (resid[:, cut] + routed[c * SEQS : (c + 1) * SEQS]).astype(BF16)
    landed(sendbuf, 1, CHIPS - 1, dsend_sem)
    landed(ybuf, 1, CHIPS - 1, rsend_sem)


def finish(packed, out, new_key, new_value, sem):
    copies = [
        pltpu.make_async_copy(packed.at[:, pl.ds(0, D)], out, sem.at[0]),
        pltpu.make_async_copy(packed.at[:, pl.ds(D, 2 * DK)], new_key, sem.at[1]),
        pltpu.make_async_copy(packed.at[:, pl.ds(D + 2 * DK, DV)], new_value, sem.at[2]),
    ]
    for copy in copies:
        copy.start()
    for copy in copies:
        copy.wait()


def per_device(
    hidden, cache_keys, cache_values, lengths, first_gain, query_weight, key_weight, value_weight, mixing, head_gain,
    out_weight, second_gain, routes, route_weight, expert_gate, expert_up, expert_down,
):
    args = (
        hidden, cache_keys, cache_values, lengths, first_gain.reshape(1, D), query_weight, key_weight, value_weight,
        mixing, head_gain.reshape(1, DV), out_weight, second_gain.reshape(1, D), routes.T, route_weight.T,
        expert_gate, expert_up, expert_down,
    )
    vmem = pltpu.VMEM
    sem = pltpu.SemaphoreType.DMA
    scratch = [
        vmem((SEQS, D), BF16), vmem((SEQS, SPAN, 2 * DK), BF16), vmem((SEQS, SPAN, DV), BF16),
        pltpu.SMEM((SEQS,), jnp.int32), vmem((1, D), F32), vmem((D, HEADS * 2 * DK), BF16), vmem((D, 2 * DK), BF16),
        vmem((D, DV), BF16), pltpu.SMEM((HEADS,), F32), vmem((1, DV), F32), vmem((HEADS * DV, D), BF16),
        vmem((1, D), F32), vmem((TOP_K, SEQS), jnp.int32), vmem((TOP_K, SEQS), F32),
        vmem((2, D, PART), BF16), vmem((2, D, PART), BF16), vmem((2, PART, D), BF16),
        vmem((SEQS, HEADS * 2 * DK), F32), vmem((SEQS, 2 * DK), F32), vmem((SEQS, DV), F32),
        vmem((GROUP * 2 * DK, 2 * LANES), BF16), vmem((SPAN, 2 * LANES), F32), vmem((LANES, SPAN), BF16), vmem((SEQS, HEADS * DV), F32), vmem((SEQS, D), F32),
        vmem((CHIPS * ROWS, PIECES * SEQS), BF16),
        vmem((2 * PIECES * SEQS, CHIPS * ROWS), BF16),
        vmem((CHIPS, ROWS, WIDTH), BF16), vmem((CHIPS, ROWS, WIDTH), BF16),
        vmem((CHIPS, ROWS, WIDTH), BF16), vmem((CHIPS, ROWS, WIDTH), BF16),
        sem((10,)), sem((WCHUNKS,)), sem((GROUPS,)), sem((GROUPS,)), sem, sem((3,)),
        sem((3,)), sem((3,)), sem, sem((BLOCKS,)), sem, sem((BLOCKS,)),
    ]
    packed = pl.pallas_call(
        kernel,
        out_shape=pltpu.VMEM((SEQS, D + 2 * DK + DV), BF16),
        in_specs=[pl.BlockSpec(memory_space=pltpu.HBM)] * len(args),
        out_specs=pl.BlockSpec(memory_space=pltpu.VMEM),
        scratch_shapes=scratch,
        compiler_params=pltpu.CompilerParams(
            collective_id=0, has_side_effects=True, vmem_limit_bytes=62 * 1024 * 1024
        ),
        name="layer",
    )(*args)
    return pl.pallas_call(
        finish,
        out_shape=(
            jax.ShapeDtypeStruct((SEQS, D), BF16),
            jax.ShapeDtypeStruct((SEQS, 2 * DK), BF16),
            jax.ShapeDtypeStruct((SEQS, DV), BF16),
        ),
        in_specs=[pl.BlockSpec(memory_space=pltpu.VMEM)],
        out_specs=[pl.BlockSpec(memory_space=pltpu.HBM)] * 3,
        scratch_shapes=[sem((3,))],
        compiler_params=pltpu.CompilerParams(vmem_limit_bytes=8 * 1024 * 1024),
        name="finish",
    )(packed)


def solution(mesh):
    return jax.shard_map(
        per_device,
        mesh=mesh,
        in_specs=(
            P("ep", None), P("ep", None, None), P("ep", None, None), P("ep"), P(), P(), P(), P(), P(), P(), P(), P(),
            P("ep", None), P("ep", None), P("ep", None, None), P("ep", None, None), P("ep", None, None),
        ),
        out_specs=(P("ep", None), P("ep", None), P("ep", None)),
        check_vma=False,
    )
```

```python
import functools

import jax
import jax.numpy as jnp
from jax import lax
from jax.experimental import pallas as pl
from jax.experimental.pallas import tpu as pltpu
from jax.sharding import PartitionSpec as P

MESH = pl.DeviceIdType.MESH
BF16 = jnp.bfloat16
F32 = jnp.float32

D = 2048
HEADS = 8
DK = 64
DV = 128
PART = 256
TOP_K = 4
SEQS = 32
SPAN = 1024
CAP = 4
CHIPS = 64
SIDE = 4
GROUP = 16
GROUPS = SEQS // GROUP
WCHUNKS = 4
PIECES = 2
WIDTH = D // PIECES
ROWS = CAP * PIECES
BLOCKS = 4
PER = CHIPS // BLOCKS
MUL = 45
INV = pow(MUL, -1, CHIPS)
LANES = GROUP * HEADS
CUT = 128
EPS = 1e-06


def dot(a, b, dims=((1,), (0,))):
    return lax.dot_general(a, b, (dims, ((), ())), preferred_element_type=F32)


def iota(shape, axis):
    return lax.broadcasted_iota(jnp.int32, shape, axis)


def row_scale(values):
    return lax.rsqrt(jnp.mean(values * values, axis=-1, keepdims=True) + EPS)


def kernel(
    hidden_h, keys_h, values_h, lengths_h, gain1_h, wq_h, wk_h, wv_h, mixing_h, hgain_h, wo_h, gain2_h,
    routes_h, rweight_h, gate_h, up_h, down_h,
    out,
    hidden, kbuf, vbuf, lens, gain1, wq, wk, wv, mixing, hgain, wo, gain2, routes, rweight, wg, wu, wd,
    qbuf, nkbuf, nvbuf, diag, scores, contrast, heads, resid, picked,
    wcomb, sendbuf, recvbuf, ybuf, retbuf,
    small_sem, wq_sem, k_sem, v_sem, wo_sem, exp_sem,
    wsend_sem, wrecv_sem, dsend_sem, drecv_sem, rsend_sem, rrecv_sem,
):
    me = lax.axis_index("ep")
    core = lax.rem(me, 2)
    chip = lax.div(me, 2)
    cx = lax.rem(chip, SIDE)
    cy = lax.rem(lax.div(chip, SIDE), SIDE)
    cz = lax.div(chip, SIDE * SIDE)
    sibling = chip * 2 + (1 - core)

    ahead_x = [lax.rem(cx + d, SIDE) * 2 + core for d in range(SIDE)]
    ahead_y = [lax.rem(cy + d, SIDE) * (SIDE * 2) for d in range(SIDE)]
    ahead_z = [lax.rem(cz + d, SIDE) * (SIDE * SIDE * 2) for d in range(SIDE)]

    def partner(k, sign):
        rel = k * INV % CHIPS
        dx, dy, dz = rel % SIDE, rel // SIDE % SIDE, rel // (SIDE * SIDE)
        return ahead_z[sign * dz % SIDE] + ahead_y[sign * dy % SIDE] + ahead_x[sign * dx % SIDE]

    smalls = [
        (routes_h, routes), (rweight_h, rweight), (hidden_h, hidden), (gain1_h, gain1), (lengths_h, lens),
        (mixing_h, mixing), (hgain_h, hgain), (gain2_h, gain2), (wk_h, wk), (wv_h, wv),
    ]
    small = [pltpu.make_async_copy(a, b, small_sem.at[i]) for i, (a, b) in enumerate(smalls)]
    for copy in small:
        copy.start()
    step = D // WCHUNKS
    wq_copies = [
        pltpu.make_async_copy(wq_h.at[pl.ds(i * step, step)], wq.at[pl.ds(i * step, step)], wq_sem.at[i])
        for i in range(WCHUNKS)
    ]
    for copy in wq_copies:
        copy.start()

    def fetch_keys(g):
        part = pl.ds(g * GROUP, GROUP)
        pltpu.make_async_copy(keys_h.at[part], kbuf.at[part], k_sem.at[g]).start()

    def fetch_values(g):
        part = pl.ds(g * GROUP, GROUP)
        pltpu.make_async_copy(values_h.at[part], vbuf.at[part], v_sem.at[g]).start()

    own = [
        pltpu.make_async_copy(gate_h.at[0], wg.at[core], exp_sem.at[0]),
        pltpu.make_async_copy(up_h.at[0], wu.at[core], exp_sem.at[1]),
        pltpu.make_async_copy(down_h.at[0], wd.at[core], exp_sem.at[2]),
    ]
    wo_copy = pltpu.make_async_copy(wo_h, wo, wo_sem)

    def fetch_own():
        for copy in own:
            copy.start()

    barrier = pltpu.get_barrier_semaphore()
    for k in range(1, CHIPS):
        pl.semaphore_signal(barrier, inc=1, device_id=(partner(k, 1),), device_id_type=MESH)
    pl.semaphore_signal(barrier, inc=1, device_id=(sibling,), device_id_type=MESH)

    lanes = PIECES * SEQS
    small[0].wait()
    small[1].wait()
    spread = (iota((SEQS, lanes), 0) == lax.rem(iota((SEQS, lanes), 1), SEQS)).astype(BF16)
    picks = dot(routes[...].astype(F32).astype(BF16), spread).astype(jnp.int32)
    lowest = jnp.min(picks, axis=0, keepdims=True)
    named = (iota((CHIPS, lanes), 0) == lowest).astype(F32)
    earlier = (iota((lanes, lanes), 0) < lax.rem(iota((lanes, lanes), 1), SEQS)).astype(F32)
    before = dot(named.astype(BF16), earlier.astype(BF16))
    place = jnp.sum(before * named, axis=0, keepdims=True).astype(jnp.int32)
    ex = lax.rem(picks, SIDE)
    ey = lax.rem(lax.div(picks, SIDE), SIDE)
    ez = lax.div(picks, SIDE * SIDE)
    offset = (
        lax.rem(ez - cz + SIDE, SIDE) * (SIDE * SIDE) + lax.rem(ey - cy + SIDE, SIDE) * SIDE + lax.rem(ex - cx + SIDE, SIDE)
    )
    piece = lax.div(iota((1, lanes), 1), SEQS)
    target = lax.rem(offset * MUL, CHIPS) * ROWS + piece * CAP + place
    high = rweight[...].astype(BF16)
    low = (rweight[...] - high.astype(F32)).astype(BF16)
    high = dot(high, spread)
    low = dot(low, spread)
    slot = iota((CHIPS * ROWS, lanes), 0)
    pick = jnp.zeros((CHIPS * ROWS, lanes), F32)
    comb_high = jnp.zeros((CHIPS * ROWS, lanes), F32)
    comb_low = jnp.zeros((CHIPS * ROWS, lanes), F32)
    for k in range(TOP_K):
        hit = slot == target[k : k + 1, :]
        pick = jnp.where(hit, 1.0, pick)
        comb_high = jnp.where(hit, high[k : k + 1, :], comb_high)
        comb_low = jnp.where(hit, low[k : k + 1, :], comb_low)
    picked[...] = pick.astype(BF16)
    wcomb[...] = jnp.transpose(jnp.concatenate([comb_high, comb_low], axis=1)).astype(BF16)

    fetch_keys(0)
    small[2].wait()
    small[3].wait()
    values = hidden[...].astype(F32)
    normed = (values * row_scale(values) * gain1[...]).astype(BF16)
    query = jnp.zeros((SEQS, HEADS * 2 * DK), F32)
    for i in range(WCHUNKS):
        wq_copies[i].wait()
        query += dot(normed[:, i * step : (i + 1) * step], wq[i * step : (i + 1) * step, :])
    qbuf[...] = query.astype(BF16).astype(F32) * DK ** (-0.5)
    for copy in small[4:]:
        copy.wait()
    new_key = dot(normed, wk[...]).astype(BF16)
    new_value = dot(normed, wv[...]).astype(BF16)
    out[:, D : D + 2 * DK] = new_key
    out[:, D + 2 * DK :] = new_value
    nkbuf[...] = new_key.astype(F32)
    nvbuf[...] = new_value.astype(F32)

    fetch_keys(1)

    def share(source, index):
        return pltpu.make_async_remote_copy(
            src_ref=source.at[core], dst_ref=source.at[core], send_sem=wsend_sem.at[index],
            recv_sem=wrecv_sem.at[index], device_id=(sibling,), device_id_type=MESH,
        )

    lane = iota((1, LANES), 1)
    lane_seq = lax.rem(lane, GROUP)
    mix = jnp.zeros((1, LANES), F32)
    for h in range(HEADS):
        mix = jnp.where(lax.div(lane, GROUP) == h, mixing[h], mix)
    row_seq = lax.rem(iota((LANES, DV), 0), GROUP)
    blank = jnp.zeros((DK, LANES), BF16)

    def prepare(g):
        first = g * GROUP
        block = jnp.concatenate(
            [qbuf[pl.ds(first, GROUP), h * 2 * DK : (h + 1) * 2 * DK] for h in range(HEADS)], axis=0
        ).T
        fresh = jnp.concatenate([nkbuf[pl.ds(first, GROUP), :]] * HEADS, axis=0).T
        limit = jnp.zeros((1, LANES), jnp.int32)
        for s in range(GROUP):
            limit = jnp.where(lane_seq == s, lens[g * GROUP + s], limit)
            one = jnp.where(lane_seq == s, block, 0.0).astype(BF16)
            for m in range(2):
                for half in range(2):
                    diag[g, s * 2 * DK + half * DK : s * 2 * DK + (half + 1) * DK, m * LANES : (m + 1) * LANES] = (
                        one[half * DK : (half + 1) * DK] if half == m else blank
                    )
        both = block * fresh
        own_score = jnp.concatenate(
            [jnp.sum(both[m * DK : (m + 1) * DK], axis=0, keepdims=True) for m in range(2)], axis=1
        )
        return jnp.concatenate([limit, limit], axis=1), own_score

    def compare(g, limit, own_score):
        first = g * GROUP
        pltpu.make_async_copy(keys_h.at[pl.ds(first, GROUP)], kbuf.at[pl.ds(first, GROUP)], k_sem.at[g]).wait()
        score = jnp.zeros((SPAN, 2 * LANES), F32)
        for s in range(0, GROUP, 2):
            pair = jnp.concatenate([kbuf[first + s], kbuf[first + s + 1]], axis=1)
            score += dot(pair, diag[g, s * 2 * DK : (s + 2) * 2 * DK])
        score = jnp.where(iota((SPAN, 2 * LANES), 0) < limit, score, -jnp.inf)
        scores[g] = score
        return jnp.maximum(jnp.max(score, axis=0, keepdims=True), own_score)

    def soften(g, highest, own_score):
        own_weight = jnp.exp(own_score - highest)
        total = own_weight
        for c in range(0, SPAN, CUT):
            weight = jnp.exp(scores[g, c : c + CUT] - highest)
            scores[g, c : c + CUT] = weight
            total += jnp.sum(weight, axis=0, keepdims=True)
        factor = jnp.concatenate([jnp.ones((1, LANES), F32), mix], axis=1) / total
        for c in range(0, SPAN, CUT):
            part = scores[g, c : c + CUT] * factor
            contrast[g, :, c : c + CUT] = (part[:, :LANES] - part[:, LANES:]).T.astype(BF16)
        own_part = own_weight * factor
        return (own_part[:, :LANES] - own_part[:, LANES:]).astype(BF16).astype(F32)

    def gather(g, own_contrast):
        first = g * GROUP
        own_rows = jnp.broadcast_to(own_contrast, (DV, LANES)).T
        mixed = own_rows * jnp.concatenate([nvbuf[pl.ds(first, GROUP), :]] * HEADS, axis=0)
        for s in range(0, GROUP, 2):
            pair = dot(contrast[g], jnp.concatenate([vbuf[first + s], vbuf[first + s + 1]], axis=1))
            mixed += jnp.where(row_seq == s, pair[:, :DV], 0.0) + jnp.where(row_seq == s + 1, pair[:, DV:], 0.0)
        normal = mixed * row_scale(mixed) * hgain[...]
        for h in range(HEADS):
            heads[pl.ds(first, GROUP), h * DV : (h + 1) * DV] = normal[h * GROUP : (h + 1) * GROUP]

    def await_values(g):
        part = pl.ds(g * GROUP, GROUP)
        pltpu.make_async_copy(values_h.at[part], vbuf.at[part], v_sem.at[g]).wait()

    limit_a, own_a = prepare(0)
    limit_b, own_b = prepare(1)
    highest_a = compare(0, limit_a, own_a)
    fetch_values(0)
    fetch_values(1)
    highest_b = compare(1, limit_b, own_b)
    wo_copy.start()
    fetch_own()
    fresh_a = soften(0, highest_a, own_a)
    await_values(0)
    gather(0, fresh_a)
    fresh_b = soften(1, highest_b, own_b)
    await_values(1)
    gather(1, fresh_b)
    pl.semaphore_wait(barrier, CHIPS)

    wo_copy.wait()
    update = dot(heads[...].astype(BF16), wo[...])
    residual = (hidden[...].astype(F32) + update).astype(BF16)
    values = residual.astype(F32)
    resid[...] = values
    given = values * row_scale(values) * gain2[...]
    stacked = jnp.concatenate([given[:, c * WIDTH : (c + 1) * WIDTH] for c in range(PIECES)], axis=0).astype(BF16)
    packed = dot(picked[...], stacked).astype(BF16).reshape(CHIPS, ROWS, WIDTH)
    sendbuf[...] = packed

    for k in range(1, CHIPS):
        pltpu.make_async_remote_copy(
            src_ref=sendbuf.at[k], dst_ref=recvbuf.at[k], send_sem=dsend_sem, recv_sem=drecv_sem.at[k // PER],
            device_id=(partner(k, 1),), device_id_type=MESH,
        ).start()
    for copy in own:
        copy.wait()
    for i, ref in enumerate((wg, wu, wd)):
        share(ref, i).start()
    recvbuf[0] = sendbuf[0]

    size = PER * ROWS
    line = iota((size, size), 0)
    column = iota((size, size), 1)

    def shuffled(a):
        return lax.rem(lax.div(a, CAP), PIECES) * (PER * CAP) + lax.div(a, ROWS) * CAP + lax.rem(a, CAP)

    to_pieces = (line == shuffled(column)).astype(BF16)
    to_messages = (shuffled(line) == column).astype(BF16)
    tall = PER * CAP

    def expert(b):
        pieces = dot(to_pieces, recvbuf[pl.ds(b * PER, PER)].reshape(size, WIDTH)).astype(BF16)
        inner = []
        for j in range(2):
            gate = jnp.zeros((tall, PART), F32)
            upper = jnp.zeros((tall, PART), F32)
            for c in range(PIECES):
                flat = pieces[c * tall : (c + 1) * tall]
                gate += dot(flat, wg[j, c * WIDTH : (c + 1) * WIDTH, :])
                upper += dot(flat, wu[j, c * WIDTH : (c + 1) * WIDTH, :])
            inner.append((gate / (1.0 + jnp.exp(-gate)) * upper).astype(BF16))
        result = []
        for c in range(PIECES):
            cut = slice(c * WIDTH, (c + 1) * WIDTH)
            result.append((dot(inner[0], wd[0, :, cut]) + dot(inner[1], wd[1, :, cut])).astype(BF16))
        ybuf[pl.ds(b * PER, PER)] = dot(to_messages, jnp.concatenate(result, axis=0)).astype(BF16).reshape(PER, ROWS, WIDTH)
        for k in range(max(b * PER, 1), (b + 1) * PER):
            pltpu.make_async_remote_copy(
                src_ref=ybuf.at[k], dst_ref=retbuf.at[k], send_sem=rsend_sem, recv_sem=rrecv_sem.at[b],
                device_id=(partner(k, -1),), device_id_type=MESH,
            ).start()

    def landed(ref, first, count, sem):
        part = ref.at[pl.ds(first, count)]
        pltpu.make_async_copy(part, part, sem).wait()

    def wait_block(ref, b, sem):
        landed(ref, max(b * PER, 1), PER - (b == 0), sem.at[b])

    for b in range(BLOCKS):
        wait_block(recvbuf, b, drecv_sem)
        if b == 0:
            for i, ref in enumerate((wg, wu, wd)):
                share(ref, i).wait()
        expert(b)
    retbuf[0] = ybuf[0]

    total = jnp.zeros((2 * lanes, WIDTH), F32)
    for b in range(BLOCKS):
        wait_block(retbuf, b, rrecv_sem)
        total += dot(wcomb[:, b * size : (b + 1) * size], retbuf[b * PER : (b + 1) * PER].reshape(size, WIDTH))
    routed = total[:lanes] + total[lanes:]
    for c in range(PIECES):
        cut = slice(c * WIDTH, (c + 1) * WIDTH)
        out[:, cut] = (resid[:, cut] + routed[c * SEQS : (c + 1) * SEQS]).astype(BF16)
    landed(sendbuf, 1, CHIPS - 1, dsend_sem)
    landed(ybuf, 1, CHIPS - 1, rsend_sem)


def finish(packed, out, new_key, new_value, sem):
    copies = [
        pltpu.make_async_copy(packed.at[:, pl.ds(0, D)], out, sem.at[0]),
        pltpu.make_async_copy(packed.at[:, pl.ds(D, 2 * DK)], new_key, sem.at[1]),
        pltpu.make_async_copy(packed.at[:, pl.ds(D + 2 * DK, DV)], new_value, sem.at[2]),
    ]
    for copy in copies:
        copy.start()
    for copy in copies:
        copy.wait()


def per_device(
    hidden, cache_keys, cache_values, lengths, first_gain, query_weight, key_weight, value_weight, mixing, head_gain,
    out_weight, second_gain, routes, route_weight, expert_gate, expert_up, expert_down,
):
    args = (
        hidden, cache_keys, cache_values, lengths, first_gain.reshape(1, D), query_weight, key_weight, value_weight,
        mixing, head_gain.reshape(1, DV), out_weight, second_gain.reshape(1, D), routes.T, route_weight.T,
        expert_gate, expert_up, expert_down,
    )
    vmem = pltpu.VMEM
    sem = pltpu.SemaphoreType.DMA
    scratch = [
        vmem((SEQS, D), BF16), vmem((SEQS, SPAN, 2 * DK), BF16), vmem((SEQS, SPAN, DV), BF16),
        pltpu.SMEM((SEQS,), jnp.int32), vmem((1, D), F32), vmem((D, HEADS * 2 * DK), BF16), vmem((D, 2 * DK), BF16),
        vmem((D, DV), BF16), pltpu.SMEM((HEADS,), F32), vmem((1, DV), F32), vmem((HEADS * DV, D), BF16),
        vmem((1, D), F32), vmem((TOP_K, SEQS), jnp.int32), vmem((TOP_K, SEQS), F32),
        vmem((2, D, PART), BF16), vmem((2, D, PART), BF16), vmem((2, PART, D), BF16),
        vmem((SEQS, HEADS * 2 * DK), F32), vmem((SEQS, 2 * DK), F32), vmem((SEQS, DV), F32),
        vmem((GROUPS, GROUP * 2 * DK, 2 * LANES), BF16), vmem((GROUPS, SPAN, 2 * LANES), F32),
        vmem((GROUPS, LANES, SPAN), BF16), vmem((SEQS, HEADS * DV), F32), vmem((SEQS, D), F32),
        vmem((CHIPS * ROWS, PIECES * SEQS), BF16),
        vmem((2 * PIECES * SEQS, CHIPS * ROWS), BF16),
        vmem((CHIPS, ROWS, WIDTH), BF16), vmem((CHIPS, ROWS, WIDTH), BF16),
        vmem((CHIPS, ROWS, WIDTH), BF16), vmem((CHIPS, ROWS, WIDTH), BF16),
        sem((10,)), sem((WCHUNKS,)), sem((GROUPS,)), sem((GROUPS,)), sem, sem((3,)),
        sem((3,)), sem((3,)), sem, sem((BLOCKS,)), sem, sem((BLOCKS,)),
    ]
    packed = pl.pallas_call(
        kernel,
        out_shape=pltpu.VMEM((SEQS, D + 2 * DK + DV), BF16),
        in_specs=[pl.BlockSpec(memory_space=pltpu.HBM)] * len(args),
        out_specs=pl.BlockSpec(memory_space=pltpu.VMEM),
        scratch_shapes=scratch,
        compiler_params=pltpu.CompilerParams(
            collective_id=0, has_side_effects=True, vmem_limit_bytes=62 * 1024 * 1024
        ),
        name="layer",
    )(*args)
    return pl.pallas_call(
        finish,
        out_shape=(
            jax.ShapeDtypeStruct((SEQS, D), BF16),
            jax.ShapeDtypeStruct((SEQS, 2 * DK), BF16),
            jax.ShapeDtypeStruct((SEQS, DV), BF16),
        ),
        in_specs=[pl.BlockSpec(memory_space=pltpu.VMEM)],
        out_specs=[pl.BlockSpec(memory_space=pltpu.HBM)] * 3,
        scratch_shapes=[sem((3,))],
        compiler_params=pltpu.CompilerParams(vmem_limit_bytes=8 * 1024 * 1024),
        name="finish",
    )(packed)


def solution(mesh):
    return jax.shard_map(
        per_device,
        mesh=mesh,
        in_specs=(
            P("ep", None), P("ep", None, None), P("ep", None, None), P("ep"), P(), P(), P(), P(), P(), P(), P(), P(),
            P("ep", None), P("ep", None), P("ep", None, None), P("ep", None, None), P("ep", None, None),
        ),
        out_specs=(P("ep", None), P("ep", None), P("ep", None)),
        check_vma=False,
    )
```

```python
import functools

import jax
import jax.numpy as jnp
from jax import lax
from jax.experimental import pallas as pl
from jax.experimental.pallas import tpu as pltpu
from jax.sharding import PartitionSpec as P

MESH = pl.DeviceIdType.MESH
BF16 = jnp.bfloat16
F32 = jnp.float32

D = 2048
HEADS = 8
DK = 64
DV = 128
PART = 256
TOP_K = 4
SEQS = 32
SPAN = 1024
CAP = 4
CHIPS = 64
SIDE = 4
GROUP = 16
GROUPS = SEQS // GROUP
WCHUNKS = 4
PIECES = 2
WIDTH = D // PIECES
ROWS = CAP * PIECES
BLOCKS = 4
PER = CHIPS // BLOCKS
MUL = 45
INV = pow(MUL, -1, CHIPS)
LANES = GROUP * HEADS
CUT = 128
EPS = 1e-06


def dot(a, b, dims=((1,), (0,))):
    return lax.dot_general(a, b, (dims, ((), ())), preferred_element_type=F32)


def iota(shape, axis):
    return lax.broadcasted_iota(jnp.int32, shape, axis)


def row_scale(values):
    return lax.rsqrt(jnp.mean(values * values, axis=-1, keepdims=True) + EPS)


def kernel(
    hidden_h, keys_h, values_h, lengths_h, gain1_h, wq_h, wk_h, wv_h, mixing_h, hgain_h, wo_h, gain2_h,
    routes_h, rweight_h, gate_h, up_h, down_h,
    out,
    hidden, kbuf, vbuf, lens, gain1, wq, wk, wv, mixing, hgain, wo, gain2, routes, rweight, wg, wu, wd,
    qbuf, nkbuf, nvbuf, diag, scores, contrast, heads, resid, picked,
    wcomb, sendbuf, recvbuf, ybuf, retbuf,
    small_sem, wq_sem, k_sem, v_sem, wo_sem, exp_sem,
    wsend_sem, wrecv_sem, dsend_sem, drecv_sem, rsend_sem, rrecv_sem,
):
    me = lax.axis_index("ep")
    core = lax.rem(me, 2)
    chip = lax.div(me, 2)
    cx = lax.rem(chip, SIDE)
    cy = lax.rem(lax.div(chip, SIDE), SIDE)
    cz = lax.div(chip, SIDE * SIDE)
    sibling = chip * 2 + (1 - core)

    ahead_x = [lax.rem(cx + d, SIDE) * 2 + core for d in range(SIDE)]
    ahead_y = [lax.rem(cy + d, SIDE) * (SIDE * 2) for d in range(SIDE)]
    ahead_z = [lax.rem(cz + d, SIDE) * (SIDE * SIDE * 2) for d in range(SIDE)]

    def partner(k, sign):
        rel = k * INV % CHIPS
        dx, dy, dz = rel % SIDE, rel // SIDE % SIDE, rel // (SIDE * SIDE)
        return ahead_z[sign * dz % SIDE] + ahead_y[sign * dy % SIDE] + ahead_x[sign * dx % SIDE]

    smalls = [
        (routes_h, routes), (rweight_h, rweight), (hidden_h, hidden), (gain1_h, gain1), (lengths_h, lens),
        (mixing_h, mixing), (hgain_h, hgain), (gain2_h, gain2), (wk_h, wk), (wv_h, wv),
    ]
    small = [pltpu.make_async_copy(a, b, small_sem.at[i]) for i, (a, b) in enumerate(smalls)]
    for copy in small:
        copy.start()
    step = D // WCHUNKS
    wq_copies = [
        pltpu.make_async_copy(wq_h.at[pl.ds(i * step, step)], wq.at[pl.ds(i * step, step)], wq_sem.at[i])
        for i in range(WCHUNKS)
    ]
    for copy in wq_copies:
        copy.start()

    def fetch_keys(g):
        part = pl.ds(g * GROUP, GROUP)
        pltpu.make_async_copy(keys_h.at[part], kbuf.at[part], k_sem.at[g]).start()

    def fetch_values(g):
        part = pl.ds(g * GROUP, GROUP)
        pltpu.make_async_copy(values_h.at[part], vbuf.at[part], v_sem.at[g]).start()

    own = [
        pltpu.make_async_copy(gate_h.at[0], wg.at[core], exp_sem.at[0]),
        pltpu.make_async_copy(up_h.at[0], wu.at[core], exp_sem.at[1]),
        pltpu.make_async_copy(down_h.at[0], wd.at[core], exp_sem.at[2]),
    ]
    wo_copy = pltpu.make_async_copy(wo_h, wo, wo_sem)

    def fetch_own():
        for copy in own:
            copy.start()

    barrier = pltpu.get_barrier_semaphore()
    for k in range(1, CHIPS):
        pl.semaphore_signal(barrier, inc=1, device_id=(partner(k, 1),), device_id_type=MESH)
    pl.semaphore_signal(barrier, inc=1, device_id=(sibling,), device_id_type=MESH)

    lanes = PIECES * SEQS
    small[0].wait()
    small[1].wait()
    spread = (iota((SEQS, lanes), 0) == lax.rem(iota((SEQS, lanes), 1), SEQS)).astype(BF16)
    picks = dot(routes[...].astype(F32).astype(BF16), spread).astype(jnp.int32)
    lowest = jnp.min(picks, axis=0, keepdims=True)
    named = (iota((CHIPS, lanes), 0) == lowest).astype(F32)
    earlier = (iota((lanes, lanes), 0) < lax.rem(iota((lanes, lanes), 1), SEQS)).astype(F32)
    before = dot(named.astype(BF16), earlier.astype(BF16))
    place = jnp.sum(before * named, axis=0, keepdims=True).astype(jnp.int32)
    ex = lax.rem(picks, SIDE)
    ey = lax.rem(lax.div(picks, SIDE), SIDE)
    ez = lax.div(picks, SIDE * SIDE)
    offset = (
        lax.rem(ez - cz + SIDE, SIDE) * (SIDE * SIDE) + lax.rem(ey - cy + SIDE, SIDE) * SIDE + lax.rem(ex - cx + SIDE, SIDE)
    )
    piece = lax.div(iota((1, lanes), 1), SEQS)
    target = lax.rem(offset * MUL, CHIPS) * ROWS + piece * CAP + place
    high = rweight[...].astype(BF16)
    low = (rweight[...] - high.astype(F32)).astype(BF16)
    high = dot(high, spread)
    low = dot(low, spread)
    slot = iota((CHIPS * ROWS, lanes), 0)
    pick = jnp.zeros((CHIPS * ROWS, lanes), F32)
    for k in range(TOP_K):
        hit = slot == target[k : k + 1, :]
        pick = jnp.where(hit, 1.0, pick)
    picked[...] = pick.astype(BF16)

    fetch_keys(0)
    small[2].wait()
    small[3].wait()
    values = hidden[...].astype(F32)
    normed = (values * row_scale(values) * gain1[...]).astype(BF16)
    query = jnp.zeros((SEQS, HEADS * 2 * DK), F32)
    for i in range(WCHUNKS):
        wq_copies[i].wait()
        query += dot(normed[:, i * step : (i + 1) * step], wq[i * step : (i + 1) * step, :])
    qbuf[...] = query.astype(BF16).astype(F32) * DK ** (-0.5)
    for copy in small[4:]:
        copy.wait()
    new_key = dot(normed, wk[...]).astype(BF16)
    new_value = dot(normed, wv[...]).astype(BF16)
    out[:, D : D + 2 * DK] = new_key
    out[:, D + 2 * DK :] = new_value
    nkbuf[...] = new_key.astype(F32)
    nvbuf[...] = new_value.astype(F32)

    fetch_keys(1)

    def share(source, index):
        return pltpu.make_async_remote_copy(
            src_ref=source.at[core], dst_ref=source.at[core], send_sem=wsend_sem.at[index],
            recv_sem=wrecv_sem.at[index], device_id=(sibling,), device_id_type=MESH,
        )

    lane = iota((1, LANES), 1)
    lane_seq = lax.rem(lane, GROUP)
    mix = jnp.zeros((1, LANES), F32)
    for h in range(HEADS):
        mix = jnp.where(lax.div(lane, GROUP) == h, mixing[h], mix)
    row_seq = lax.rem(iota((LANES, DV), 0), GROUP)
    blank = jnp.zeros((DK, LANES), BF16)

    def prepare(g):
        first = g * GROUP
        block = jnp.concatenate(
            [qbuf[pl.ds(first, GROUP), h * 2 * DK : (h + 1) * 2 * DK] for h in range(HEADS)], axis=0
        ).T
        fresh = jnp.concatenate([nkbuf[pl.ds(first, GROUP), :]] * HEADS, axis=0).T
        limit = jnp.zeros((1, LANES), jnp.int32)
        for s in range(GROUP):
            limit = jnp.where(lane_seq == s, lens[g * GROUP + s], limit)
            one = jnp.where(lane_seq == s, block, 0.0).astype(BF16)
            for m in range(2):
                for half in range(2):
                    diag[g, s * 2 * DK + half * DK : s * 2 * DK + (half + 1) * DK, m * LANES : (m + 1) * LANES] = (
                        one[half * DK : (half + 1) * DK] if half == m else blank
                    )
        both = block * fresh
        own_score = jnp.concatenate(
            [jnp.sum(both[m * DK : (m + 1) * DK], axis=0, keepdims=True) for m in range(2)], axis=1
        )
        return jnp.concatenate([limit, limit], axis=1), own_score

    def compare(g, limit, own_score):
        first = g * GROUP
        pltpu.make_async_copy(keys_h.at[pl.ds(first, GROUP)], kbuf.at[pl.ds(first, GROUP)], k_sem.at[g]).wait()
        score = jnp.zeros((SPAN, 2 * LANES), F32)
        for s in range(0, GROUP, 2):
            pair = jnp.concatenate([kbuf[first + s], kbuf[first + s + 1]], axis=1)
            score += dot(pair, diag[g, s * 2 * DK : (s + 2) * 2 * DK])
        score = jnp.where(iota((SPAN, 2 * LANES), 0) < limit, score, -jnp.inf)
        scores[g] = score
        return jnp.maximum(jnp.max(score, axis=0, keepdims=True), own_score)

    def soften(g, highest, own_score):
        own_weight = jnp.exp(own_score - highest)
        total = own_weight
        for c in range(0, SPAN, CUT):
            weight = jnp.exp(scores[g, c : c + CUT] - highest)
            scores[g, c : c + CUT] = weight
            total += jnp.sum(weight, axis=0, keepdims=True)
        factor = jnp.concatenate([jnp.ones((1, LANES), F32), mix], axis=1) / total
        for c in range(0, SPAN, CUT):
            part = scores[g, c : c + CUT] * factor
            contrast[g, :, c : c + CUT] = (part[:, :LANES] - part[:, LANES:]).T.astype(BF16)
        own_part = own_weight * factor
        return (own_part[:, :LANES] - own_part[:, LANES:]).astype(BF16).astype(F32)

    def gather(g, own_contrast):
        first = g * GROUP
        own_rows = jnp.broadcast_to(own_contrast, (DV, LANES)).T
        mixed = own_rows * jnp.concatenate([nvbuf[pl.ds(first, GROUP), :]] * HEADS, axis=0)
        for s in range(0, GROUP, 2):
            pair = dot(contrast[g], jnp.concatenate([vbuf[first + s], vbuf[first + s + 1]], axis=1))
            mixed += jnp.where(row_seq == s, pair[:, :DV], 0.0) + jnp.where(row_seq == s + 1, pair[:, DV:], 0.0)
        normal = mixed * row_scale(mixed) * hgain[...]
        for h in range(HEADS):
            heads[pl.ds(first, GROUP), h * DV : (h + 1) * DV] = normal[h * GROUP : (h + 1) * GROUP]

    def await_values(g):
        part = pl.ds(g * GROUP, GROUP)
        pltpu.make_async_copy(values_h.at[part], vbuf.at[part], v_sem.at[g]).wait()

    limit_a, own_a = prepare(0)
    limit_b, own_b = prepare(1)
    highest_a = compare(0, limit_a, own_a)
    fetch_values(0)
    fetch_values(1)
    highest_b = compare(1, limit_b, own_b)
    wo_copy.start()
    fetch_own()
    fresh_a = soften(0, highest_a, own_a)
    await_values(0)
    fresh_b = soften(1, highest_b, own_b)
    gather(0, fresh_a)
    await_values(1)
    gather(1, fresh_b)
    pl.semaphore_wait(barrier, CHIPS)

    wo_copy.wait()
    update = dot(heads[...].astype(BF16), wo[...])
    residual = (hidden[...].astype(F32) + update).astype(BF16)
    values = residual.astype(F32)
    resid[...] = values
    given = values * row_scale(values) * gain2[...]
    stacked = jnp.concatenate([given[:, c * WIDTH : (c + 1) * WIDTH] for c in range(PIECES)], axis=0).astype(BF16)
    packed = dot(picked[...], stacked).astype(BF16).reshape(CHIPS, ROWS, WIDTH)
    sendbuf[...] = packed

    for k in range(1, CHIPS):
        pltpu.make_async_remote_copy(
            src_ref=sendbuf.at[k], dst_ref=recvbuf.at[k], send_sem=dsend_sem, recv_sem=drecv_sem.at[k // PER],
            device_id=(partner(k, 1),), device_id_type=MESH,
        ).start()
    for copy in own:
        copy.wait()
    for i, ref in enumerate((wg, wu, wd)):
        share(ref, i).start()
    recvbuf[0] = sendbuf[0]
    comb_high = jnp.zeros((CHIPS * ROWS, lanes), F32)
    comb_low = jnp.zeros((CHIPS * ROWS, lanes), F32)
    for k in range(TOP_K):
        hit = slot == target[k : k + 1, :]
        comb_high = jnp.where(hit, high[k : k + 1, :], comb_high)
        comb_low = jnp.where(hit, low[k : k + 1, :], comb_low)
    wcomb[...] = jnp.transpose(jnp.concatenate([comb_high, comb_low], axis=1)).astype(BF16)

    size = PER * ROWS
    line = iota((size, size), 0)
    column = iota((size, size), 1)

    def shuffled(a):
        return lax.rem(lax.div(a, CAP), PIECES) * (PER * CAP) + lax.div(a, ROWS) * CAP + lax.rem(a, CAP)

    to_pieces = (line == shuffled(column)).astype(BF16)
    to_messages = (shuffled(line) == column).astype(BF16)
    tall = PER * CAP

    def expert(b):
        pieces = dot(to_pieces, recvbuf[pl.ds(b * PER, PER)].reshape(size, WIDTH)).astype(BF16)
        inner = []
        for j in range(2):
            gate = jnp.zeros((tall, PART), F32)
            upper = jnp.zeros((tall, PART), F32)
            for c in range(PIECES):
                flat = pieces[c * tall : (c + 1) * tall]
                gate += dot(flat, wg[j, c * WIDTH : (c + 1) * WIDTH, :])
                upper += dot(flat, wu[j, c * WIDTH : (c + 1) * WIDTH, :])
            inner.append((gate / (1.0 + jnp.exp(-gate)) * upper).astype(BF16))
        result = []
        for c in range(PIECES):
            cut = slice(c * WIDTH, (c + 1) * WIDTH)
            result.append((dot(inner[0], wd[0, :, cut]) + dot(inner[1], wd[1, :, cut])).astype(BF16))
        ybuf[pl.ds(b * PER, PER)] = dot(to_messages, jnp.concatenate(result, axis=0)).astype(BF16).reshape(PER, ROWS, WIDTH)
        for k in range(max(b * PER, 1), (b + 1) * PER):
            pltpu.make_async_remote_copy(
                src_ref=ybuf.at[k], dst_ref=retbuf.at[k], send_sem=rsend_sem, recv_sem=rrecv_sem.at[b],
                device_id=(partner(k, -1),), device_id_type=MESH,
            ).start()

    def landed(ref, first, count, sem):
        part = ref.at[pl.ds(first, count)]
        pltpu.make_async_copy(part, part, sem).wait()

    def wait_block(ref, b, sem):
        landed(ref, max(b * PER, 1), PER - (b == 0), sem.at[b])

    for b in range(BLOCKS):
        wait_block(recvbuf, b, drecv_sem)
        if b == 0:
            for i, ref in enumerate((wg, wu, wd)):
                share(ref, i).wait()
        expert(b)
    retbuf[0] = ybuf[0]

    total = jnp.zeros((2 * lanes, WIDTH), F32)
    for b in range(BLOCKS):
        wait_block(retbuf, b, rrecv_sem)
        total += dot(wcomb[:, b * size : (b + 1) * size], retbuf[b * PER : (b + 1) * PER].reshape(size, WIDTH))
    routed = total[:lanes] + total[lanes:]
    for c in range(PIECES):
        cut = slice(c * WIDTH, (c + 1) * WIDTH)
        out[:, cut] = (resid[:, cut] + routed[c * SEQS : (c + 1) * SEQS]).astype(BF16)
    landed(sendbuf, 1, CHIPS - 1, dsend_sem)
    landed(ybuf, 1, CHIPS - 1, rsend_sem)


def finish(packed, out, new_key, new_value, sem):
    copies = [
        pltpu.make_async_copy(packed.at[:, pl.ds(0, D)], out, sem.at[0]),
        pltpu.make_async_copy(packed.at[:, pl.ds(D, 2 * DK)], new_key, sem.at[1]),
        pltpu.make_async_copy(packed.at[:, pl.ds(D + 2 * DK, DV)], new_value, sem.at[2]),
    ]
    for copy in copies:
        copy.start()
    for copy in copies:
        copy.wait()


def per_device(
    hidden, cache_keys, cache_values, lengths, first_gain, query_weight, key_weight, value_weight, mixing, head_gain,
    out_weight, second_gain, routes, route_weight, expert_gate, expert_up, expert_down,
):
    args = (
        hidden, cache_keys, cache_values, lengths, first_gain.reshape(1, D), query_weight, key_weight, value_weight,
        mixing, head_gain.reshape(1, DV), out_weight, second_gain.reshape(1, D), routes.T, route_weight.T,
        expert_gate, expert_up, expert_down,
    )
    vmem = pltpu.VMEM
    sem = pltpu.SemaphoreType.DMA
    scratch = [
        vmem((SEQS, D), BF16), vmem((SEQS, SPAN, 2 * DK), BF16), vmem((SEQS, SPAN, DV), BF16),
        pltpu.SMEM((SEQS,), jnp.int32), vmem((1, D), F32), vmem((D, HEADS * 2 * DK), BF16), vmem((D, 2 * DK), BF16),
        vmem((D, DV), BF16), pltpu.SMEM((HEADS,), F32), vmem((1, DV), F32), vmem((HEADS * DV, D), BF16),
        vmem((1, D), F32), vmem((TOP_K, SEQS), jnp.int32), vmem((TOP_K, SEQS), F32),
        vmem((2, D, PART), BF16), vmem((2, D, PART), BF16), vmem((2, PART, D), BF16),
        vmem((SEQS, HEADS * 2 * DK), F32), vmem((SEQS, 2 * DK), F32), vmem((SEQS, DV), F32),
        vmem((GROUPS, GROUP * 2 * DK, 2 * LANES), BF16), vmem((GROUPS, SPAN, 2 * LANES), F32),
        vmem((GROUPS, LANES, SPAN), BF16), vmem((SEQS, HEADS * DV), F32), vmem((SEQS, D), F32),
        vmem((CHIPS * ROWS, PIECES * SEQS), BF16),
        vmem((2 * PIECES * SEQS, CHIPS * ROWS), BF16),
        vmem((CHIPS, ROWS, WIDTH), BF16), vmem((CHIPS, ROWS, WIDTH), BF16),
        vmem((CHIPS, ROWS, WIDTH), BF16), vmem((CHIPS, ROWS, WIDTH), BF16),
        sem((10,)), sem((WCHUNKS,)), sem((GROUPS,)), sem((GROUPS,)), sem, sem((3,)),
        sem((3,)), sem((3,)), sem, sem((BLOCKS,)), sem, sem((BLOCKS,)),
    ]
    packed = pl.pallas_call(
        kernel,
        out_shape=pltpu.VMEM((SEQS, D + 2 * DK + DV), BF16),
        in_specs=[pl.BlockSpec(memory_space=pltpu.HBM)] * len(args),
        out_specs=pl.BlockSpec(memory_space=pltpu.VMEM),
        scratch_shapes=scratch,
        compiler_params=pltpu.CompilerParams(
            collective_id=0, has_side_effects=True, vmem_limit_bytes=62 * 1024 * 1024
        ),
        name="layer",
    )(*args)
    return pl.pallas_call(
        finish,
        out_shape=(
            jax.ShapeDtypeStruct((SEQS, D), BF16),
            jax.ShapeDtypeStruct((SEQS, 2 * DK), BF16),
            jax.ShapeDtypeStruct((SEQS, DV), BF16),
        ),
        in_specs=[pl.BlockSpec(memory_space=pltpu.VMEM)],
        out_specs=[pl.BlockSpec(memory_space=pltpu.HBM)] * 3,
        scratch_shapes=[sem((3,))],
        compiler_params=pltpu.CompilerParams(vmem_limit_bytes=8 * 1024 * 1024),
        name="finish",
    )(packed)


def solution(mesh):
    return jax.shard_map(
        per_device,
        mesh=mesh,
        in_specs=(
            P("ep", None), P("ep", None, None), P("ep", None, None), P("ep"), P(), P(), P(), P(), P(), P(), P(), P(),
            P("ep", None), P("ep", None), P("ep", None, None), P("ep", None, None), P("ep", None, None),
        ),
        out_specs=(P("ep", None), P("ep", None), P("ep", None)),
        check_vma=False,
    )
```
